256 devices in a mesh: sp: 32 (over z, x), fs: 4 (over y), tp: 2 (over core).
Axes of the slice: x: 4, y: 4, z: 8, core: 2. Of those that a mesh axis runs over, the one named last changes fastest.
Arguments:
- tokens: bfloat16 [4, 4096, 2048], P('fs', 'sp', 'tp'), may hold values from -6 to 6
- norm_gain: float32 [2048], replicated, may hold values from 0.1 to 1.9
- retain_query: bfloat16 [2048, 512], P('fs', 'tp'), may hold values from -0.125 to 0.125
- retain_key: bfloat16 [2048, 512], P('fs', 'tp'), may hold values from -0.125 to 0.125
- retain_value: bfloat16 [2048, 1024], P('fs', 'tp'), may hold values from -0.125 to 0.125
- retain_gate: bfloat16 [2048, 1024], P('fs', 'tp'), may hold values from -0.125 to 0.125
- differ_query: bfloat16 [2048, 1024], P('fs', 'tp'), may hold values from -0.125 to 0.125
- differ_key: bfloat16 [2048, 1024], P('fs', 'tp'), may hold values from -0.125 to 0.125
- differ_value: bfloat16 [2048, 1024], P('fs', 'tp'), may hold values from -0.125 to 0.125
- log_decay: float32 [4, 4096, 4], P('fs', 'sp', 'tp'), may hold values from -0.8 to 0
- lambdas: float32 [8], P('tp'), may hold values from 0.3 to 0.8
- query_gain: float32 [8, 2, 64], P('tp'), may hold values from 1 to 9
- key_gain: float32 [8, 2, 64], P('tp'), may hold values from 1 to 9
- retain_gain: float32 [1024], P('tp'), may hold values from 0.1 to 1.9
- differ_gain: float32 [1024], P('tp'), may hold values from 0.1 to 1.9
- retain_out: bfloat16 [1024, 2048], P('tp', 'fs'), may hold values from -0.1875 to 0.1875
- differ_out: bfloat16 [1024, 2048], P('tp', 'fs'), may hold values from -0.1875 to 0.1875
Outputs:
- mixed: bfloat16 [4, 4096, 2048], P('fs', ('sp', 'tp'))
The draws below stay inside these ranges and needn't reach their ends.
All inputs are finite; a program needn't handle non-finite values.
Results may differ from the reference program's by a relative error of at most 0.014.
The reference program's roundings to bfloat16 on the way count: a program that leaves them out, or rounds other values in their place, can miss the bound.
Values may be sent and summed in bfloat16 or wider, within the bound.
A program may use at most 128 MiB of HBM per device.

```python
import math
import jax
import jax.numpy as jnp
from jax import lax

D = 2048
RETENTION_HEADS = 4
RET_DK = 128
RET_DV = 256
DIFF_HEADS = 8
DIFF_HD = 64
DIFF_DV = 128
GRID_W = 64
TOK_DEV = 128
SEQUENCE_COUNT = 4
SEQUENCE_LENGTH = 4096
N_TP = 2


def draw_log_decay(key, part):
    random_subkeys = jax.random.split(jax.random.fold_in(key, 11), 6)
    blocks = SEQUENCE_LENGTH // TOK_DEV
    fast_share = 0.5
    fast_heads = jax.random.uniform(random_subkeys[0], (SEQUENCE_COUNT, 1, RETENTION_HEADS)) < fast_share
    fast_rates = jnp.exp(jax.random.uniform(random_subkeys[1], (SEQUENCE_COUNT, 1, RETENTION_HEADS), minval=math.log(1.0 / 60.0), maxval=math.log(1.0 / 25.0)))
    decay_rates = jnp.where(fast_heads, fast_rates, 0.8 / SEQUENCE_LENGTH)
    decay_factors = jnp.exp(jax.random.uniform(random_subkeys[2], (SEQUENCE_COUNT, blocks, 1, RETENTION_HEADS), minval=math.log(0.5), maxval=math.log(2.0)))
    decay_factors = (decay_factors * jnp.ones((1, 1, TOK_DEV, 1), jnp.float32)).reshape(SEQUENCE_COUNT, SEQUENCE_LENGTH, RETENTION_HEADS)
    leading_location = jax.random.randint(random_subkeys[3], (SEQUENCE_COUNT, 1, RETENTION_HEADS), 0, SEQUENCE_LENGTH)
    distance_location = jax.random.randint(random_subkeys[4], (SEQUENCE_COUNT, 1, RETENTION_HEADS), 1, SEQUENCE_LENGTH)
    spike_locations = jnp.concatenate([leading_location, (leading_location + distance_location) % SEQUENCE_LENGTH], axis=1)
    spike_penalty = jax.random.uniform(random_subkeys[5], (SEQUENCE_COUNT, 2, RETENTION_HEADS), minval=math.log(0.5), maxval=math.log(0.8))
    spike_mask = jnp.arange(SEQUENCE_LENGTH, dtype=jnp.int32)[None, :, None, None] == spike_locations[:, None, :, :]
    spike_values = jnp.sum(jnp.where(spike_mask, spike_penalty[:, None, :, :], 0.0), axis=2)
    return (-(decay_rates * decay_factors) + spike_values).astype(jnp.float32)


def draw_gain_common(key, salt):
    base_gain = jax.random.uniform(jax.random.fold_in(key, salt), (DIFF_HEADS, 2, DIFF_HD), minval=1.05, maxval=1.6)
    return base_gain.astype(jnp.float32)


def draw_query_gain(key, part):
    return draw_gain_common(key, 1)


def draw_key_gain(key, part):
    return draw_gain_common(key, 2)


def steps_of(rng, extent, pieces, low, top_value):
    def one(position, parts):
        draws = jax.random.uniform(jax.random.fold_in(jax.random.fold_in(rng, 6), position), (parts,), jnp.float32, low / len(pieces), top_value / len(pieces))
        return jnp.repeat(jnp.exp(draws), extent[position] // parts).reshape((-1,) + (1,) * (len(extent) - position - 1))

    level = one(*pieces[0])
    for cut in pieces[1:]:
        level = level * one(*cut)
    return level


def centred(own_key, dims, width, reach, cuts=(), kind=jnp.bfloat16):
    values = width * jax.random.normal(own_key, dims, jnp.float32)
    if cuts:
        values = values * steps_of(own_key, dims, cuts, -0.22, 0.18)
    return jnp.clip(values, -reach, reach).astype(kind)


def setup_inputs(seed: int = 0) -> dict:
    splits = jax.random.split(jax.random.key(seed), 18)
    return {
        "tokens": centred(splits[0], (SEQUENCE_COUNT, SEQUENCE_LENGTH, D), 1.0, 6.0, ((0, 4), (1, 32), (2, 2))),
        "norm_gain": jnp.clip(1.0 + 0.18 * jax.random.normal(splits[1], (D,), jnp.float32), 0.1, 1.9),
        "retain_query": centred(splits[2], (D, RETENTION_HEADS * RET_DK), D ** -0.5, 0.125, ((0, 4), (1, 2))),
        "retain_key": centred(splits[3], (D, RETENTION_HEADS * RET_DK), D ** -0.5, 0.125, ((0, 4), (1, 2))),
        "retain_value": centred(splits[4], (D, RETENTION_HEADS * RET_DV), D ** -0.5, 0.125, ((0, 4), (1, 2))),
        "retain_gate": centred(splits[5], (D, RETENTION_HEADS * RET_DV), D ** -0.5, 0.125, ((0, 4), (1, 2))),
        "differ_query": centred(splits[6], (D, DIFF_HEADS * 2 * DIFF_HD), D ** -0.5, 0.125, ((0, 4), (1, 2))),
        "differ_key": centred(splits[7], (D, DIFF_HEADS * 2 * DIFF_HD), D ** -0.5, 0.125, ((0, 4), (1, 2))),
        "differ_value": centred(splits[8], (D, DIFF_HEADS * DIFF_DV), D ** -0.5, 0.125, ((0, 4), (1, 2))),
        "log_decay": draw_log_decay(jax.random.fold_in(splits[17], 71), 0),
        "lambdas": jnp.clip(0.3 + 0.5 * jax.random.uniform(splits[10], (DIFF_HEADS,), jnp.float32) ** steps_of(splits[10], (DIFF_HEADS,), ((0, 2),), -0.2, 0.2), 0.3, 0.8),
        "query_gain": draw_query_gain(jax.random.fold_in(splits[17], 71), 0),
        "key_gain": draw_key_gain(jax.random.fold_in(splits[17], 71), 0),
        "retain_gain": jnp.clip(1.0 + 0.18 * jax.random.normal(splits[13], (RETENTION_HEADS * RET_DV,), jnp.float32), 0.1, 1.9),
        "differ_gain": jnp.clip(1.0 + 0.18 * jax.random.normal(splits[14], (DIFF_HEADS * DIFF_DV,), jnp.float32), 0.1, 1.9),
        "retain_out": centred(splits[15], (RETENTION_HEADS * RET_DV, D), (RETENTION_HEADS * RET_DV) ** -0.5, 0.1875, ((0, 2), (1, 4))),
        "differ_out": centred(splits[16], (DIFF_HEADS * DIFF_DV, D), (DIFF_HEADS * DIFF_DV) ** -0.5, 0.1875, ((0, 2), (1, 4))),
    }


EPSILON = 1e-06
ROPE_BASE = 10000.0
HIGHEST = lax.Precision.HIGHEST

def rotate_half(vector, positions):
    length = vector.shape[-1]
    inverse = jnp.power(ROPE_BASE, -jnp.arange(0, length, 2, dtype=jnp.float32) / length)
    angles = positions.astype(jnp.float32)[:, None] * inverse[None, :]
    target_shape = (positions.shape[0],) + (1,) * (vector.ndim - 2) + (length // 2,)
    cosine = jnp.cos(angles).reshape(target_shape)
    sine_part = jnp.sin(angles).reshape(target_shape)
    leading = vector[..., :length // 2]
    trailing = vector[..., length // 2:]
    return jnp.concatenate([leading * cosine - trailing * sine_part, trailing * cosine + leading * sine_part], axis=-1)

def rotary_grid(vector, positions):
    middle = vector.shape[-1] // 2
    return jnp.concatenate([rotate_half(vector[..., :middle], positions // GRID_W), rotate_half(vector[..., middle:], positions % GRID_W)], axis=-1)

def rms_scale(vector, gain_row):
    return vector * lax.rsqrt(lax.optimization_barrier(jnp.mean(vector * vector, axis=-1, keepdims=True)) + EPSILON) * gain_row

def retention_branch(retention_query, retention_keys, retention_values, retention_gate, log_decay, retain_gain):
    blocks = SEQUENCE_LENGTH // TOK_DEV

    def shaped(array):
        return array.reshape((blocks, TOK_DEV) + array.shape[1:])
    sources = (shaped(retention_query), shaped(retention_keys), shaped(retention_values), shaped(log_decay))
    zeros_state = jnp.zeros((RETENTION_HEADS, RET_DK, RET_DV), jnp.float32)

    def forward(states, segment):
        block_query, block_keys, block_values, block_decay = segment
        levels = jnp.cumsum(block_decay, axis=0)
        final_level = levels[-1]
        query_wide = block_query.astype(jnp.float32)
        key_wide = block_keys.astype(jnp.float32)
        value_wide = block_values.astype(jnp.float32)
        scores = jnp.einsum('thd,shd->hts', query_wide, key_wide)
        nearness = jnp.exp(-jnp.abs(levels.T[:, :, None] - levels.T[:, None, :]))
        weights = lax.optimization_barrier((scores * nearness).astype(jnp.bfloat16)).astype(jnp.float32)
        inside = jnp.einsum('hts,shv->thv', weights, value_wide)
        before = jnp.einsum('thd,hdv->thv', query_wide * jnp.exp(levels)[..., None], states, precision=HIGHEST)
        own = jnp.einsum('shd,shv->hdv', key_wide * jnp.exp(final_level - levels)[..., None], value_wide, precision=HIGHEST)
        states = states * jnp.exp(final_level)[:, None, None] + own
        return (states, inside + before)

    def backward(states, segment):
        block_query, block_keys, block_values, block_decay = segment
        levels = jnp.cumsum(block_decay, axis=0)
        final_level = levels[-1]
        query_wide = block_query.astype(jnp.float32)
        key_wide = block_keys.astype(jnp.float32)
        value_wide = block_values.astype(jnp.float32)
        behind = jnp.einsum('thd,hdv->thv', query_wide * jnp.exp(final_level - levels)[..., None], states, precision=HIGHEST)
        own = jnp.einsum('shd,shv->hdv', key_wide * jnp.exp(levels)[..., None], value_wide, precision=HIGHEST)
        states = own + jnp.exp(final_level)[:, None, None] * states
        return (states, behind)
    ignored, leading = lax.scan(forward, zeros_state, sources)
    ignored, trailing = lax.scan(backward, zeros_state, sources, reverse=True)
    combined = (leading + trailing).reshape(SEQUENCE_LENGTH, RETENTION_HEADS, RET_DV)
    scaled = rms_scale(combined, retain_gain.reshape(RETENTION_HEADS, RET_DV))
    return (jax.nn.silu(retention_gate.astype(jnp.float32)) * scaled.reshape(SEQUENCE_LENGTH, -1)).astype(jnp.bfloat16)

def contrast_branch(contrast_query, contrast_keys, contrast_values, lambdas, differ_gain):
    blocks = SEQUENCE_LENGTH // TOK_DEV
    key_wide = contrast_keys.astype(jnp.float32)
    value_wide = contrast_values.astype(jnp.float32)

    def attend(block_query):
        scores = jnp.einsum('qhmd,khmd->mhqk', block_query.astype(jnp.float32), key_wide) * DIFF_HD ** (-0.5)
        maxima = lax.optimization_barrier(jnp.max(scores, axis=-1, keepdims=True))
        exponent = jnp.exp(scores - maxima)
        totals = lax.optimization_barrier(jnp.sum(exponent, axis=-1))
        rounded = lax.optimization_barrier(exponent.astype(jnp.bfloat16)).astype(jnp.float32)
        numerators = jnp.einsum('mhqk,khv->mhqv', rounded, value_wide)
        ratios = numerators / totals[..., None]
        contrast_mix = ratios[0] - lambdas[:, None, None] * ratios[1]
        return jnp.transpose(contrast_mix, (1, 0, 2))
    query_blocks = contrast_query.reshape((blocks, TOK_DEV) + contrast_query.shape[1:])
    combined = lax.map(attend, query_blocks).reshape(SEQUENCE_LENGTH, DIFF_HEADS, DIFF_DV)
    scaled = rms_scale(combined, differ_gain.reshape(DIFF_HEADS, DIFF_DV))
    return scaled.reshape(SEQUENCE_LENGTH, -1).astype(jnp.bfloat16)

def reference(tokens, norm_gain, retain_query, retain_key, retain_value, retain_gate, differ_query, differ_key, differ_value, log_decay, lambdas, query_gain, key_gain, retain_gain, differ_gain, retain_out, differ_out):

    def one_sequence(paired):
        sequence_rows, decay_rows = paired
        normed = rms_scale(sequence_rows.astype(jnp.float32), norm_gain).astype(jnp.bfloat16)
        positions = jnp.arange(SEQUENCE_LENGTH, dtype=jnp.int32)

        def project(matrix):
            return jnp.dot(normed, matrix, preferred_element_type=jnp.float32)
        retention_query = rotary_grid(project(retain_query).reshape(SEQUENCE_LENGTH, RETENTION_HEADS, RET_DK), positions).astype(jnp.bfloat16)
        retention_keys = (rotary_grid(project(retain_key).reshape(SEQUENCE_LENGTH, RETENTION_HEADS, RET_DK), positions) * RET_DK ** (-0.5)).astype(jnp.bfloat16)
        retention_values = project(retain_value).astype(jnp.bfloat16).reshape(SEQUENCE_LENGTH, RETENTION_HEADS, RET_DV)
        retention_gate = project(retain_gate).astype(jnp.bfloat16)
        contrast_query = rotary_grid(rms_scale(project(differ_query).reshape(SEQUENCE_LENGTH, DIFF_HEADS, 2, DIFF_HD), query_gain), positions).astype(jnp.bfloat16)
        contrast_keys = rotary_grid(rms_scale(project(differ_key).reshape(SEQUENCE_LENGTH, DIFF_HEADS, 2, DIFF_HD), key_gain), positions).astype(jnp.bfloat16)
        contrast_values = project(differ_value).astype(jnp.bfloat16).reshape(SEQUENCE_LENGTH, DIFF_HEADS, DIFF_DV)
        retention_features = retention_branch(retention_query, retention_keys, retention_values, retention_gate, decay_rows, retain_gain)
        contrast_features = contrast_branch(contrast_query, contrast_keys, contrast_values, lambdas, differ_gain)
        retain_width = RETENTION_HEADS * RET_DV // N_TP
        differ_width = DIFF_HEADS * DIFF_DV // N_TP
        summed = jnp.zeros((SEQUENCE_LENGTH, D), jnp.float32)
        for group in range(N_TP):
            partial_value = jnp.dot(retention_features[:, group * retain_width:(group + 1) * retain_width], retain_out[group * retain_width:(group + 1) * retain_width], preferred_element_type=jnp.float32)
            partial_value = partial_value + jnp.dot(contrast_features[:, group * differ_width:(group + 1) * differ_width], differ_out[group * differ_width:(group + 1) * differ_width], preferred_element_type=jnp.float32)
            summed = summed + lax.optimization_barrier(partial_value.astype(jnp.bfloat16)).astype(jnp.float32)
        return summed.astype(jnp.bfloat16)
    return lax.map(one_sequence, (tokens, log_decay))
```

```python
import functools

import numpy as np
import jax
import jax.numpy as jnp
from jax import lax
from jax.experimental import pallas as pl
from jax.experimental.pallas import tpu as pltpu
from jax.sharding import PartitionSpec as P

F32 = jnp.float32
BF16 = jnp.bfloat16
MESH = pl.DeviceIdType.MESH
EPS = 1e-06
ROPE_BASE = 10000.0
NX, NY, NZ = 4, 4, 8
ROWS = 128
BLOCK = NX * ROWS
D = 2048
WIDTHS = (256, 256, 256, 128)

TOK = 0
PART = 4
WG = 8
WO1 = 24
WO2 = 28
DEC = 40
KV = 43
ST = 59
DF = 75
GT = 78
RM = 81
OUT = 84
COPIES = 88
LOCALS = 16


def rope_tables():
    lane = np.arange(128)
    value = np.arange(64, dtype=np.float64)[:, None]
    tables = []
    for group in (32, 64):
        inverse = ROPE_BASE ** (-2.0 * ((lane % group) % (group // 2)) / group)
        angle = value * inverse[None, :]
        sign = np.where((lane % group) < group // 2, -1.0, 1.0)[None, :]
        tables += [np.cos(angle), np.sin(angle) * sign]
    return np.stack(tables).astype(np.float32)


def kernel(
    tok_in, w_rq, w_rk, w_rv, w_rg, w_dq, w_dk, w_dv, w_ro, w_do, dec_in, par, gain_in, tab,
    out,
    tok, xn, wg0, wg1, wg2, wg3, wo, dec, kb, vb, st, dz, cosd, sind, cosr, sinr, proj, qbd,
    m_run, l_run, acc, rq, rk, rv, grow, gcol, mix, gate, feat, df, gt, rm, fall, part, pin,
    ssem, rsem, lsem,
):
    sp = lax.axis_index("sp")
    z, x = sp // NX, sp % NX
    y = lax.axis_index("fs")
    c = lax.axis_index("tp")
    other = 1 - c

    def along_x(i):
        return {"sp": z * NX + i}

    def along_y(i):
        return {"fs": i}

    def along_z(i):
        return {"sp": i * NX + x}

    partner = {"tp": other}
    xs = [x, (x + 1) % NX, (x + 2) % NX, (x + 3) % NX]
    ys = [y, (y + 1) % NY, (y + 2) % NY, (y + 3) % NY]
    zr, zl = (z + 1) % NZ, (z + NZ - 1) % NZ

    def remote(i, src, dst, device):
        return pltpu.make_async_remote_copy(
            src_ref=src, dst_ref=dst, send_sem=ssem.at[i], recv_sem=rsem.at[i],
            device_id=device, device_id_type=MESH,
        )

    sent = []

    def send(i, src, dst, device):
        copy = remote(i, src, dst, device)
        copy.start()
        sent.append(copy)

    def arrived(i, ref):
        remote(i, ref, ref, partner).wait_recv()

    class Ring4:
        def __init__(self, base, at, device, full, half):
            self.base, self.at, self.device, self.full, self.half = base, at, device, full, half

        def own(self):
            block = self.full(self.at[0])
            send(self.base, block, block, self.device(self.at[1]))
            send(self.base + 1, block, block, self.device(self.at[3]))

        def forward(self):
            arrived(self.base, self.full(self.at[3]))
            a = self.half(self.at[3], 0)
            send(self.base + 2, a, a, self.device(self.at[1]))
            arrived(self.base + 1, self.full(self.at[1]))
            b = self.half(self.at[1], 1)
            send(self.base + 3, b, b, self.device(self.at[3]))

        def far(self):
            arrived(self.base + 2, self.half(self.at[2], 0))
            arrived(self.base + 3, self.half(self.at[2], 1))

    wgs = (wg0, wg1, wg2, wg3)
    token_ring = Ring4(
        TOK, xs, along_x,
        lambda i: tok.at[i, c],
        lambda i, h: tok.at[i, c, pl.ds(h * 64, 64)],
    )

    def weight_ring(g):
        ref = wgs[g]
        return Ring4(
            WG + 4 * g, ys, along_y,
            lambda i: ref.at[pl.ds(pl.multiple_of(i * 512, 512), 512)],
            lambda i, h: ref.at[pl.ds(pl.multiple_of(i * 512 + h * 256, 256), 256)],
        )

    rings = [weight_ring(g) for g in range(4)]
    out_ring1 = Ring4(
        WO1, ys, along_y,
        lambda i: wo.at[i, x],
        lambda i, h: wo.at[i, x, pl.ds(h * 128, 128)],
    )

    def out_ring2(k):
        yy = ys[k]
        return Ring4(
            WO2 + 4 * (k - 1), xs, along_x,
            lambda i: wo.at[yy, i],
            lambda i, h: wo.at[yy, i, pl.ds(h * 128, 128)],
        )

    rings2 = {k: out_ring2(k) for k in (1, 2, 3)}

    def local(i, src, dst):
        copy = pltpu.make_async_copy(src, dst, lsem.at[i])
        copy.start()
        return copy

    col = pl.ds(pl.multiple_of(x * 128, 128), 128)
    col2 = pl.ds(pl.multiple_of((x // 2) * 128, 128), 128)
    own_rows = pl.ds(pl.multiple_of(y * 512, 512), 512)
    lo, hi = pl.ds(0, 128), pl.ds(128, 128)
    load_tok = local(0, tok_in.at[0], tok.at[x, c])
    load_g = [
        [local(1, w_dk.at[:, col], wg0.at[own_rows, lo]), local(2, w_dv.at[:, col], wg0.at[own_rows, hi])],
        [local(3, w_dq.at[:, col], wg1.at[own_rows, lo]), local(4, w_rq.at[:, col2], wg1.at[own_rows, hi])],
        [local(5, w_rk.at[:, col2], wg2.at[own_rows, lo]), local(6, w_rv.at[:, col], wg2.at[own_rows, hi])],
        [local(7, w_rg.at[:, col], wg3.at[own_rows])],
    ]
    load_o = []
    for i in range(NX):
        load_o.append(local(8 + 2 * i, w_ro.at[pl.ds(i * 128, 128)], wo.at[y, i, lo]))
        load_o.append(local(9 + 2 * i, w_do.at[pl.ds(i * 128, 128)], wo.at[y, i, hi]))

    barrier = pltpu.get_barrier_semaphore()
    peers = [along_x(xs[1]), along_x(xs[2]), along_x(xs[3]), along_y(ys[1]), along_y(ys[3]),
             along_z(zr), along_z(zl), partner]
    for peer in peers:
        pl.semaphore_signal(barrier, inc=1, device_id=peer, device_id_type=MESH)
    pl.semaphore_wait(barrier, len(peers))

    load_tok.wait()
    token_ring.own()
    send(PART, tok.at[x, c], tok.at[x, c], partner)
    for copy in load_g[0]:
        copy.wait()
    rings[0].own()
    for d in (1, 2, 3):
        send(DEC + d - 1, dec_in, dec.at[x], along_x(xs[d]))
    dec[x] = dec_in[...]
    for group in load_g[1:]:
        for copy in group:
            copy.wait()
    for copy in load_o:
        copy.wait()

    lane = lax.broadcasted_iota(jnp.int32, (128, 128), 1)
    sub = lax.broadcasted_iota(jnp.int32, (128, 128), 0)

    lane64 = lax.broadcasted_iota(jnp.int32, (64, 128), 1)
    zrow = pl.ds(pl.multiple_of(z * 8, 8), 8)
    for k, ref in enumerate((cosd, sind, cosr, sinr)):
        by_row = tab[k, zrow, :]
        by_col = tab[k]
        is_row = (lane64 % 64) < 32 if k < 2 else lane64 < 64
        for b in range(8):
            ref[b * 64 : b * 64 + 64, :] = jnp.where(is_row, by_row[b : b + 1, :], by_col)

    def rope(u, cos, sin, group):
        half = group // 2
        up = pltpu.roll(u, 128 - half, 1)
        down = pltpu.roll(u, half, 1)
        return u * cos + jnp.where((lane % group) < half, up, down) * sin

    def map_norm(u, gain):
        square = u * u
        first = jnp.sum(jnp.where(lane < 64, square, 0.0), axis=-1, keepdims=True)
        second = jnp.sum(jnp.where(lane < 64, 0.0, square), axis=-1, keepdims=True)
        scale = jnp.where(
            lane < 64, lax.rsqrt(first / 64 + EPS), lax.rsqrt(second / 64 + EPS)
        )
        return u * scale * gain

    def normalize(i):
        def rows(j, carry):
            r = pl.ds(pl.multiple_of(j * 16, 16), 16)
            w = pl.ds(pl.multiple_of(i * 128 + j * 16, 16), 16)
            a = tok[i, 0, r, :].astype(F32)
            b = tok[i, 1, r, :].astype(F32)
            total = jnp.sum(a * a, axis=-1, keepdims=True) + jnp.sum(b * b, axis=-1, keepdims=True)
            scale = lax.rsqrt(total / D + EPS)
            xn[w, 0:1024] = (a * scale * gain_in[:, 0:1024]).astype(BF16)
            xn[w, 1024:2048] = (b * scale * gain_in[:, 1024:2048]).astype(BF16)
            return carry

        lax.fori_loop(0, 8, rows, 0)

    def project(g):
        ref = wgs[g]
        width = WIDTHS[g]

        def rows(j, carry):
            r = pl.ds(pl.multiple_of(j * 256, 256), 256)
            proj[r, 0:width] = jnp.dot(xn[r, :], ref[...], preferred_element_type=F32)
            return carry

        lax.fori_loop(0, 2, rows, 0)

    rings[0].forward()
    rings[1].own()
    out_ring1.own()

    token_ring.forward()
    send(PART + 1, tok.at[xs[3], c], tok.at[xs[3], c], partner)
    send(PART + 2, tok.at[xs[1], c], tok.at[xs[1], c], partner)
    arrived(PART, tok.at[x, other])
    normalize(xs[0])
    arrived(PART + 1, tok.at[xs[3], other])
    normalize(xs[3])
    arrived(PART + 2, tok.at[xs[1], other])
    normalize(xs[1])
    token_ring.far()
    send(PART + 3, tok.at[xs[2], c], tok.at[xs[2], c], partner)
    arrived(PART + 3, tok.at[xs[2], other])
    normalize(xs[2])

    rings[0].far()
    project(0)
    kgain = par[1:2, :]
    for i in range(NX):
        r = slice(i * 128, i * 128 + 128)
        u = map_norm(proj[r, 0:128], kgain)
        kb[z, r, :] = rope(u, cosd[r, :], sind[r, :], 32).astype(BF16)
        vb[z, :, r] = proj[r, 128:256].T.astype(BF16)

    zs = [(z + NZ + d) % NZ for d in range(-4, 5)]

    def at_z(d):
        return zs[d + 4]

    def kv_send(step, way, piece):
        origin = at_z(-step if way == 0 else step)
        ref = (kb, vb)[piece].at[origin]
        send(KV + 4 * step + 2 * way + piece, ref, ref, along_z(zr if way == 0 else zl))

    def kv_arrived(step, way, piece):
        origin = at_z(-(step + 1) if way == 0 else step + 1)
        arrived(KV + 4 * step + 2 * way + piece, (kb, vb)[piece].at[origin])

    for piece in (0, 1):
        for way in (0, 1):
            kv_send(0, way, piece)

    for d in (1, 2, 3):
        arrived(DEC + d - 1, dec.at[xs[4 - d]])
    lane8 = lax.broadcasted_iota(jnp.int32, (8, 128), 1)
    offset = jnp.zeros((1, 1), F32)
    head = x // 2
    for b in range(NX):
        level = dec[b]
        for k in (1, 2, 4, 8, 16, 32, 64):
            level = level + jnp.where(lane8 >= k, pltpu.roll(level, k, 1), 0.0)
        row = jnp.where(head == 0, level[0:1, :], level[1:2, :]) + offset
        offset = row[:, 127:128]
        grow[:, b * 128 : b * 128 + 128] = row
        gcol[b * 128 : b * 128 + 128, :] = jnp.broadcast_to(row, (128, 128)).T
    dz[z] = jnp.broadcast_to(offset, (8, 128))

    rings[1].forward()
    rings[2].own()
    rings[1].far()
    project(1)
    qgain = par[0:1, :]
    for i in range(NX):
        r = slice(i * 128, i * 128 + 128)
        u = map_norm(proj[r, 0:128], qgain)
        u = rope(u, cosd[r, :], sind[r, :], 32).astype(BF16).astype(F32) * 0.125
        u = u.T
        s = slice((i % 2) * 128, (i % 2) * 128 + 128)
        qbd[i // 2, :, s] = jnp.where(sub < 64, u, 0.0).astype(BF16)
        qbd[2 + i // 2, :, s] = jnp.where(sub < 64, 0.0, u).astype(BF16)
        rq[r, :] = rope(proj[r, 128:256], cosr[r, :], sinr[r, :], 64).astype(BF16)

    m_run[...] = jnp.full((4, 1, 256), -jnp.inf, F32)
    l_run[...] = jnp.zeros((4, 1, 256), F32)
    acc[...] = jnp.zeros((4, 128, 256), F32)

    def attend(origin):
        def tile(q, carry):
            s = jnp.dot(kb[origin], qbd[q], preferred_element_type=F32)
            before = m_run[q]
            now = jnp.maximum(before, jnp.max(s, axis=0, keepdims=True))
            shrink = jnp.exp(before - now)
            e = jnp.exp(s - now)
            m_run[q] = now
            l_run[q] = l_run[q] * shrink + jnp.sum(e, axis=0, keepdims=True)
            acc[q] = acc[q] * shrink + jnp.dot(
                vb[origin], e.astype(BF16), preferred_element_type=F32
            )
            return carry

        lax.fori_loop(0, 4, tile, 0)

    attend(z)

    out_ring1.forward()
    rings[3].own()
    rings2[1].own()
    rings2[3].own()

    def kv_step(step):
        for piece in (0, 1):
            for way in (0, 1):
                kv_arrived(step, way, piece)
                if step < 2 or (step == 2 and piece == way):
                    kv_send(step + 1, way, piece)

    kv_step(0)
    attend(at_z(-1))
    attend(at_z(1))
    out_ring1.far()
    rings2[2].own()
    kv_step(1)
    attend(at_z(-2))
    attend(at_z(2))
    rings2[1].forward()
    rings2[3].forward()
    rings[2].forward()
    rings[2].far()
    project(2)
    for i in range(NX):
        r = slice(i * 128, i * 128 + 128)
        u = rope(proj[r, 0:128], cosr[r, :], sinr[r, :], 64) * (128 ** -0.5)
        rk[r, :] = u.astype(BF16)
        rv[r, :] = proj[r, 128:256].astype(BF16)
    end = dz[z][0:1, :]
    forward_state = jnp.zeros((128, 128), F32)
    backward_state = jnp.zeros((128, 128), F32)
    for i in range(NX):
        r = slice(i * 128, i * 128 + 128)
        key = rk[r, :].astype(F32)
        value = rv[r, :]
        level = gcol[r, :]
        a = (key * jnp.exp(end - level)).T.astype(BF16)
        b = (key * jnp.exp(level)).T.astype(BF16)
        forward_state += jnp.dot(a, value, preferred_element_type=F32)
        backward_state += jnp.dot(b, value, preferred_element_type=F32)
    st[z, 0] = forward_state.astype(BF16)
    st[z, 1] = backward_state.astype(BF16)

    def st_send(step, way):
        origin = at_z(-step if way == 0 else step)
        device = along_z(zr if way == 0 else zl)
        base = ST + 4 * step + 2 * way
        states = st.at[origin] if step < 3 else st.at[origin, way]
        send(base, states, states, device)
        if step < 3 or way == 1:
            send(base + 1, dz.at[origin], dz.at[origin], device)

    def st_step(step):
        for way in (0, 1):
            origin = at_z(-(step + 1) if way == 0 else step + 1)
            base = ST + 4 * step + 2 * way
            arrived(base, st.at[origin] if step < 3 else st.at[origin, way])
            if step < 3 or way == 1:
                arrived(base + 1, dz.at[origin])
            if step < 3:
                st_send(step + 1, way)

    st_send(0, 0)
    st_send(0, 1)

    kv_step(2)
    attend(at_z(-3))
    rings[3].forward()
    rings2[2].forward()
    attend(at_z(3))
    st_step(0)

    for i in range(NX):
        r = slice(i * 128, i * 128 + 128)
        s = lax.dot_general(rq[r, :], rk[...], (((1,), (1,)), ((), ())), preferred_element_type=F32)
        level = jnp.concatenate([gcol[r, :]] * 4, axis=1)
        w = (s * jnp.exp(-jnp.abs(level - grow[...]))).astype(BF16)
        mix[i] = jnp.dot(w, rv[...], preferred_element_type=F32)

    st_step(1)
    rings[3].far()
    project(3)
    for i in range(NX):
        gate[i] = proj[i * 128 : i * 128 + 128, 0:128].astype(BF16)
    for d in (1, 2, 3):
        send(GT + d - 1, gate.at[xs[d]], gt.at[x], along_x(xs[d]))
    gt[x] = gate[x]

    st_step(2)
    kv_arrived(3, 0, 0)
    kv_arrived(3, 1, 1)
    attend(at_z(4))

    lam = par[3:4, 0:1]
    dgain = par[2:3, :]
    for t in range(2):
        first = acc[t] / l_run[t]
        second = acc[2 + t] / l_run[2 + t]
        both = first - lam * second
        both = both * lax.rsqrt(jnp.mean(both * both, axis=0, keepdims=True) + EPS)
        for h in range(2):
            feat[2 * t + h] = (both[:, h * 128 : h * 128 + 128].T * dgain).astype(BF16)
    for d in (1, 2, 3):
        send(DF + d - 1, feat.at[xs[d]], df.at[x], along_x(xs[d]))
    df[x] = feat[x]

    st_step(3)
    forward_state = jnp.zeros((128, 128), F32)
    total = jnp.zeros((1, 128), F32)
    for k in range(NZ - 1, -1, -1):
        take = jnp.where(k < z, 1.0, 0.0)
        forward_state += (jnp.exp(total) * take) * st[k, 0].astype(F32)
        total += dz[k][0:1, :] * take
    backward_state = jnp.zeros((128, 128), F32)
    total = jnp.zeros((1, 128), F32)
    for k in range(NZ):
        take = jnp.where(k > z, 1.0, 0.0)
        backward_state += (jnp.exp(total) * take) * st[k, 1].astype(F32)
        total += dz[k][0:1, :] * take
    states = jnp.concatenate([forward_state, backward_state], axis=0).astype(BF16)
    for i in range(NX):
        r = slice(i * 128, i * 128 + 128)
        query = rq[r, :].astype(F32)
        level = gcol[r, :]
        q2 = jnp.concatenate(
            [(query * jnp.exp(level)).astype(BF16), (query * jnp.exp(end - level)).astype(BF16)],
            axis=1,
        )
        mix[i] = mix[i] + jnp.dot(q2, states, preferred_element_type=F32)
    for d in (1, 2, 3):
        send(RM + d - 1, mix.at[xs[d]], rm.at[x], along_x(xs[d]))
    rm[x] = mix[x]

    for k in (1, 3, 2):
        rings2[k].far()
    for d in (1, 2, 3):
        arrived(GT + d - 1, gt.at[xs[4 - d]])
        arrived(DF + d - 1, df.at[xs[4 - d]])
        arrived(RM + d - 1, rm.at[xs[4 - d]])
    for h in range(2):
        a, b = rm[2 * h], rm[2 * h + 1]
        total = jnp.sum(a * a, axis=-1, keepdims=True) + jnp.sum(b * b, axis=-1, keepdims=True)
        scale = lax.rsqrt(total / 256 + EPS)
        for k, m in ((2 * h, a), (2 * h + 1, b)):
            g = gt[k].astype(F32)
            value = (g * jax.nn.sigmoid(g)) * (m * scale * par[4 + k : 5 + k, :])
            fall[:, k * 256 : k * 256 + 128] = value.astype(BF16)
            fall[:, k * 256 + 128 : k * 256 + 256] = df[k]

    mine = pl.ds(pl.multiple_of(c * 64, 64), 64)
    theirs = pl.ds(pl.multiple_of(other * 64, 64), 64)
    for k in range(NY):
        w = wo[k].reshape(1024, 512)
        part[k] = jnp.dot(fall[...], w, preferred_element_type=F32).astype(BF16)
        send(OUT + k, part.at[k, theirs], pin.at[k], partner)
    for k in range(NY):
        arrived(OUT + k, pin.at[k])
        value = part[k, mine, :].astype(F32) + pin[k].astype(F32)
        out[0, :, k * 512 : k * 512 + 512] = value.astype(BF16)
    for copy in sent:
        copy.wait_send()


def body(
    tokens, norm_gain, retain_query, retain_key, retain_value, retain_gate, differ_query,
    differ_key, differ_value, log_decay, lambdas, query_gain, key_gain, retain_gain,
    differ_gain, retain_out, differ_out,
):
    x = lax.axis_index("sp") % NX
    own = lambda a: lax.dynamic_slice_in_dim(a, x, 1, 0)
    par = jnp.concatenate(
        [
            own(query_gain.reshape(4, 128)),
            own(key_gain.reshape(4, 128)),
            own(differ_gain.reshape(4, 128)),
            own(jnp.broadcast_to(lambdas[:, None], (4, 128))),
            retain_gain.reshape(4, 128),
        ],
        axis=0,
    )
    dec = jnp.pad(log_decay[0].T, ((0, 6), (0, 0)))
    tab = jnp.asarray(rope_tables())
    anywhere = pl.BlockSpec(memory_space=pl.ANY)
    vmem = pl.BlockSpec(memory_space=pltpu.VMEM)
    V = pltpu.VMEM
    return pl.pallas_call(
        kernel,
        out_shape=jax.ShapeDtypeStruct((1, 64, D), BF16),
        in_specs=[anywhere] * 10 + [vmem] * 4,
        out_specs=vmem,
        scratch_shapes=[
            V((NX, 2, 128, 1024), BF16),
            V((BLOCK, D), BF16),
            V((D, 256), BF16), V((D, 256), BF16), V((D, 256), BF16), V((D, 128), BF16),
            V((NY, NX, 256, 512), BF16),
            V((NX, 8, 128), F32),
            V((NZ, BLOCK, 128), BF16),
            V((NZ, 128, BLOCK), BF16),
            V((NZ, 2, 128, 128), BF16),
            V((NZ, 8, 128), F32),
            V((BLOCK, 128), F32), V((BLOCK, 128), F32), V((BLOCK, 128), F32), V((BLOCK, 128), F32),
            V((BLOCK, 256), F32),
            V((4, 128, 256), BF16),
            V((4, 1, 256), F32), V((4, 1, 256), F32), V((4, 128, 256), F32),
            V((BLOCK, 128), BF16), V((BLOCK, 128), BF16), V((BLOCK, 128), BF16),
            V((1, BLOCK), F32), V((BLOCK, 128), F32),
            V((NX, 128, 128), F32),
            V((NX, 128, 128), BF16), V((NX, 128, 128), BF16),
            V((NX, 128, 128), BF16), V((NX, 128, 128), BF16), V((NX, 128, 128), F32),
            V((128, 1024), BF16),
            V((NY, 128, 512), BF16), V((NY, 64, 512), BF16),
            pltpu.SemaphoreType.DMA((COPIES,)),
            pltpu.SemaphoreType.DMA((COPIES,)),
            pltpu.SemaphoreType.DMA((LOCALS,)),
        ],
        compiler_params=pltpu.CompilerParams(
            collective_id=0, has_side_effects=True, vmem_limit_bytes=48 * 1024 * 1024
        ),
    )(
        tokens, retain_query, retain_key, retain_value, retain_gate, differ_query, differ_key,
        differ_value, retain_out, differ_out, dec, par, norm_gain.reshape(1, D), tab,
    )


def solution(mesh):
    in_specs = (
        P("fs", "sp", "tp"), P(),
        P("fs", "tp"), P("fs", "tp"), P("fs", "tp"), P("fs", "tp"), P("fs", "tp"), P("fs", "tp"), P("fs", "tp"),
        P("fs", "sp", "tp"),
        P("tp"), P("tp", None, None), P("tp", None, None), P("tp"), P("tp"),
        P("tp", "fs"), P("tp", "fs"),
    )
    out_specs = P("fs", ("sp", "tp"), None)
    return jax.shard_map(body, mesh=mesh, in_specs=in_specs, out_specs=out_specs, check_vma=False)
```

```python
import functools

import numpy as np
import jax
import jax.numpy as jnp
from jax import lax
from jax.experimental import pallas as pl
from jax.experimental.pallas import tpu as pltpu
from jax.sharding import PartitionSpec as P

F32 = jnp.float32
BF16 = jnp.bfloat16
MESH = pl.DeviceIdType.MESH
EPS = 1e-06
ROPE_BASE = 10000.0
NX, NY, NZ = 4, 4, 8
ROWS = 128
BLOCK = NX * ROWS
D = 2048
WIDTHS = (256, 256, 256, 128)

TOK = 0
PART = 8
W0 = 16
W1 = 24
W2 = 28
W3 = 32
OY = 36
OZ = 40
OX = 48
DEC = 56
KV = 59
ST = 75
DF = 91
GT = 94
RM = 97
OUT = 100
COPIES = 104
LOCALS = 24


def rope_tables():
    lane = np.arange(128)
    value = np.arange(64, dtype=np.float64)[:, None]
    tables = []
    for group in (32, 64):
        inverse = ROPE_BASE ** (-2.0 * ((lane % group) % (group // 2)) / group)
        angle = value * inverse[None, :]
        sign = np.where((lane % group) < group // 2, -1.0, 1.0)[None, :]
        tables += [np.cos(angle), np.sin(angle) * sign]
    return np.stack(tables).astype(np.float32)


class Phases:
    def __init__(self):
        self.scope = None

    def __call__(self, name):
        if self.scope is not None:
            self.scope.__exit__(None, None, None)
        self.scope = jax.named_scope(name) if name else None
        if self.scope is not None:
            self.scope.__enter__()


def kernel(
    tok_in, w_rq, w_rk, w_rv, w_rg, w_dq, w_dk, w_dv, w_ro, w_do,
    dec_hbm, lam_hbm, qgain_hbm, kgain_hbm, rgain_hbm, dgain_hbm, ngain_hbm, tab_hbm,
    out,
    dec_in, lam_in, qgain_in, kgain_in, rgain_in, dgain_in, gain_in, tab, tok, xn, wg0, wg1, wg2, wg3, wo, dec, kb, vb, st, dz, cosd, sind, cosr, sinr, proj, qbd,
    m_run, l_run, acc, rq, rk, rv, grow, gcol, mix, gate, feat, df, gt, rm, fall, part, pin,
    ssem, rsem, lsem,
):
    phase = Phases()
    sp = lax.axis_index("sp")
    z, x = sp // NX, sp % NX
    y = lax.axis_index("fs")
    c = lax.axis_index("tp")
    other = 1 - c

    def along_x(i):
        return {"sp": z * NX + i}

    def along_y(i):
        return {"fs": i}

    def along_z(i):
        return {"sp": i * NX + x}

    partner = {"tp": other}
    xs = [x, (x + 1) % NX, (x + 2) % NX, (x + 3) % NX]
    ys = [y, (y + 1) % NY, (y + 2) % NY, (y + 3) % NY]
    zr, zl = (z + 1) % NZ, (z + NZ - 1) % NZ

    def remote(i, src, dst, device):
        return pltpu.make_async_remote_copy(
            src_ref=src, dst_ref=dst, send_sem=ssem.at[i], recv_sem=rsem.at[i],
            device_id=device, device_id_type=MESH,
        )

    sent = []

    def send(i, src, dst, device):
        copy = remote(i, src, dst, device)
        copy.start()
        sent.append(copy)

    def arrived(i, ref):
        remote(i, ref, ref, partner).wait_recv()

    class Ring4:
        def __init__(self, base, right, left, own, to_right, to_left, half, onward, far):
            self.base, self.right, self.left = base, right, left
            self.src, self.to_right, self.to_left, self.half = own, to_right, to_left, half
            self.onward, self.far_half = onward, far

        def own(self):
            send(self.base, self.src, self.to_right, self.right)
            send(self.base + 1, self.src, self.to_left, self.left)

        def near(self):
            self.from_left()
            self.from_right()

        def from_left(self):
            arrived(self.base, self.half[2])
            send(self.base + 2, self.half[0], self.onward[0], self.right)

        def from_right(self):
            arrived(self.base + 1, self.half[3])
            send(self.base + 3, self.half[1], self.onward[1], self.left)

        def far(self):
            arrived(self.base + 2, self.far_half[0])
            arrived(self.base + 3, self.far_half[1])

    def ring_at(base, at, sides, full, half):
        return Ring4(
            base, sides[0], sides[1], full(at[0]), full(at[0]), full(at[0]),
            (half(at[3], 0), half(at[1], 1), full(at[3]), full(at[1])),
            (half(at[3], 0), half(at[1], 1)), (half(at[2], 0), half(at[2], 1)),
        )

    wgs = (wg0, wg1, wg2, wg3)
    def rows_of(start, size):
        return pl.ds(pl.multiple_of(start, size & -size), size)

    token_rings = [
        ring_at(
            TOK + 4 * piece, xs, (along_x(xs[1]), along_x(xs[3])),
            lambda i, p=piece: tok.at[i, c, pl.ds(p * 64, 64)],
            lambda i, h, p=piece: tok.at[i, c, pl.ds(p * 64 + h * 32, 32)],
        )
        for piece in (0, 1)
    ]

    def weight_ring(base, ref, start, size):
        return ring_at(
            base, ys, (along_y(ys[1]), along_y(ys[3])),
            lambda i: ref.at[rows_of(i * 512 + start, size)],
            lambda i, h: ref.at[rows_of(i * 512 + start + h * (size // 2), size // 2)],
        )

    ring0 = [weight_ring(W0 + 4 * piece, wg0, piece * 256, 256) for piece in (0, 1)]
    ring1 = weight_ring(W1, wg1, 0, 512)
    ring2 = weight_ring(W2, wg2, 0, 512)
    ring3 = weight_ring(W3, wg3, 0, 512)

    zc = z % 4
    zcs = [(zc + d) % 4 for d in range(4)]

    def slice_of(slot, i, h=None):
        if h is None:
            return wo.at[slot, x, rows_of(i * 64, 64)]
        return wo.at[slot, x, rows_of(i * 64 + h * 32, 32)]

    out_y = Ring4(
        OY, along_y(ys[1]), along_y(ys[3]), slice_of(0, zc), slice_of(2, zc), slice_of(1, zc),
        (slice_of(2, zc, 0), slice_of(1, zc, 1), slice_of(2, zc), slice_of(1, zc)),
        (slice_of(3, zc, 0), slice_of(3, zc, 1)), (slice_of(3, zc, 0), slice_of(3, zc, 1)),
    )

    near, far = pl.ds(1, 2), 3
    out_z = []
    out_x = []
    for k, slot in enumerate((near, far)):
        piece = functools.partial(slice_of, slot)
        out_z.append(ring_at(OZ + 4 * k, zcs, (along_z(zr), along_z(zl)), piece, piece))
        out_x.append(
            ring_at(
                OX + 4 * k, xs, (along_x(xs[1]), along_x(xs[3])),
                lambda i, s=slot: wo.at[s, i],
                lambda i, h, s=slot: wo.at[s, i, pl.ds(h * 128, 128)],
            )
        )

    def local(i, src, dst):
        copy = pltpu.make_async_copy(src, dst, lsem.at[i])
        copy.start()
        return copy

    col = pl.ds(pl.multiple_of(x * 128, 128), 128)
    col2 = pl.ds(pl.multiple_of((x // 2) * 128, 128), 128)
    own_rows = pl.ds(pl.multiple_of(y * 512, 512), 512)
    lo, hi = pl.ds(0, 128), pl.ds(128, 128)
    load_tok = local(0, tok_in.at[0], tok.at[x, c])
    load_g = [
        [local(1, w_dk.at[:, col], wg0.at[own_rows, lo]), local(2, w_dv.at[:, col], wg0.at[own_rows, hi])],
        [local(3, w_dq.at[:, col], wg1.at[own_rows, lo]), local(4, w_rq.at[:, col2], wg1.at[own_rows, hi])],
        [local(5, w_rk.at[:, col2], wg2.at[own_rows, lo]), local(6, w_rv.at[:, col], wg2.at[own_rows, hi])],
        [local(7, w_rg.at[:, col], wg3.at[own_rows])],
    ]
    load_o = []
    for i in range(NX):
        load_o.append(local(8 + 2 * i, w_ro.at[pl.ds(i * 128, 128)], wo.at[0, i, lo]))
        load_o.append(local(9 + 2 * i, w_do.at[pl.ds(i * 128, 128)], wo.at[0, i, hi]))

    load_small = [
        local(16 + i, src, dst)
        for i, (src, dst) in enumerate((
            (dec_hbm, dec_in), (lam_hbm, lam_in), (qgain_hbm, qgain_in), (kgain_hbm, kgain_in),
            (rgain_hbm, rgain_in), (dgain_hbm, dgain_in), (ngain_hbm, gain_in), (tab_hbm, tab),
        ))
    ]

    phase("barrier")
    barrier = pltpu.get_barrier_semaphore()
    peers = [along_x(xs[1]), along_x(xs[2]), along_x(xs[3]), along_y(ys[1]), along_y(ys[3]),
             along_z(zr), along_z(zl), partner]
    for peer in peers:
        pl.semaphore_signal(barrier, inc=1, device_id=peer, device_id_type=MESH)
    pl.semaphore_wait(barrier, len(peers))

    phase("loads")
    load_tok.wait()
    for ring in token_rings:
        ring.own()
    send(PART, tok.at[x, c], tok.at[x, c], partner)
    for copy in load_g[0]:
        copy.wait()
    ring0[0].own()
    for copy in load_o:
        copy.wait()
    out_y.own()
    ring0[1].own()
    for copy in load_small:
        copy.wait()
    for d in (1, 2, 3):
        send(DEC + d - 1, dec_in, dec.at[x], along_x(xs[d]))
    dec[x] = dec_in[...]
    for group in load_g[1:]:
        for copy in group:
            copy.wait()

    lane = lax.broadcasted_iota(jnp.int32, (128, 128), 1)
    sub = lax.broadcasted_iota(jnp.int32, (128, 128), 0)

    phase("tables")
    lane64 = lax.broadcasted_iota(jnp.int32, (64, 128), 1)
    zrow = pl.ds(pl.multiple_of(z * 8, 8), 8)
    for k, ref in enumerate((cosd, sind, cosr, sinr)):
        by_row = tab[k, zrow, :]
        by_col = tab[k]
        is_row = (lane64 % 64) < 32 if k < 2 else lane64 < 64
        for b in range(8):
            ref[b * 64 : b * 64 + 64, :] = jnp.where(is_row, by_row[b : b + 1, :], by_col)

    def rope(u, cos, sin, group):
        half = group // 2
        up = pltpu.roll(u, 128 - half, 1)
        down = pltpu.roll(u, half, 1)
        return u * cos + jnp.where((lane % group) < half, up, down) * sin

    def map_norm(u, gain):
        square = u * u
        first = jnp.sum(jnp.where(lane < 64, square, 0.0), axis=-1, keepdims=True)
        second = jnp.sum(jnp.where(lane < 64, 0.0, square), axis=-1, keepdims=True)
        scale = jnp.where(
            lane < 64, lax.rsqrt(first / 64 + EPS), lax.rsqrt(second / 64 + EPS)
        )
        return u * scale * gain

    order = [xs[0], xs[3], xs[1], xs[2]]

    def block_rows(j):
        return rows_of(order[j] * 128, 128)

    def normalize(j):
        i = order[j]
        for k in range(8):
            r = slice(k * 16, k * 16 + 16)
            w = slice(j * 128 + k * 16, j * 128 + k * 16 + 16)
            a = tok[i, 0, r, :].astype(F32)
            b = tok[i, 1, r, :].astype(F32)
            total = jnp.sum(a * a, axis=-1, keepdims=True) + jnp.sum(b * b, axis=-1, keepdims=True)
            scale = lax.rsqrt(total / D + EPS)
            xn[w, 0:1024] = (a * scale * gain_in[:, 0:1024]).astype(BF16)
            xn[w, 1024:2048] = (b * scale * gain_in[:, 1024:2048]).astype(BF16)

    def project(g, start=0, size=BLOCK):
        ref = wgs[g]
        width = WIDTHS[g]
        step = 256 if size % 256 == 0 else 128
        for j in range(start, start + size, step):
            proj[j : j + step, 0:width] = jnp.dot(
                xn[j : j + step, :], ref[...], preferred_element_type=F32
            )

    def part_send(n, block, start, size):
        ref = tok.at[block, c, pl.ds(start, size)]
        send(PART + n, ref, ref, partner)

    def part_arrived(n, block, start, size):
        arrived(PART + n, tok.at[block, other, pl.ds(start, size)])

    kgain = jnp.concatenate([kgain_in[x][0:1, :], kgain_in[x][1:2, :]], axis=1)

    def keys_values(j):
        r = slice(j * 128, j * 128 + 128)
        a = block_rows(j)
        u = map_norm(proj[r, 0:128], kgain)
        kb[z, r, :] = rope(u, cosd[a, :], sind[a, :], 32).astype(BF16)
        vb[z, :, r] = proj[r, 128:256].T.astype(BF16)

    phase("w0a")
    ring0[0].near()
    phase("tok_a")
    token_rings[0].near()
    part_send(1, order[1], 0, 64)
    part_send(2, order[2], 0, 64)
    phase("oy")
    out_y.near()
    out_z[0].own()
    phase("w0b")
    ring0[1].near()
    ring1.own()
    phase("tok_b")
    token_rings[1].near()
    part_send(3, order[1], 64, 64)
    part_send(4, order[2], 64, 64)
    phase("norm0")
    arrived(PART, tok.at[x, other])
    normalize(0)
    phase("norm1")
    part_arrived(1, order[1], 0, 64)
    part_arrived(3, order[1], 64, 64)
    normalize(1)
    phase("tok_far_a")
    token_rings[0].far()
    part_send(5, order[3], 0, 64)
    phase("oz_near")
    out_z[0].near()
    phase("norm2")
    part_arrived(2, order[2], 0, 64)
    part_arrived(4, order[2], 64, 64)
    normalize(2)
    phase("tok_far_b")
    token_rings[1].far()
    part_send(6, order[3], 64, 64)
    phase("oy_far")
    out_y.far()
    out_z[1].own()
    phase("w0_far")
    ring0[0].far()
    ring0[1].far()
    phase("project0")
    project(0, 0, 384)
    phase("kv_post")
    for j in range(3):
        keys_values(j)
    phase("norm3")
    part_arrived(5, order[3], 0, 64)
    part_arrived(6, order[3], 64, 64)
    normalize(3)
    phase("project0b")
    project(0, 384, 128)
    keys_values(3)

    zs = [(z + NZ + d) % NZ for d in range(-4, 5)]

    def at_z(d):
        return zs[d + 4]

    def kv_send(step, way, piece):
        origin = at_z(-step if way == 0 else step)
        ref = (kb, vb)[piece].at[origin]
        send(KV + 4 * step + 2 * way + piece, ref, ref, along_z(zr if way == 0 else zl))

    def kv_arrived(step, way, piece):
        origin = at_z(-(step + 1) if way == 0 else step + 1)
        arrived(KV + 4 * step + 2 * way + piece, (kb, vb)[piece].at[origin])

    for piece in (0, 1):
        for way in (0, 1):
            kv_send(0, way, piece)

    phase("levels")
    for d in (1, 2, 3):
        arrived(DEC + d - 1, dec.at[xs[4 - d]])
    lane8 = lax.broadcasted_iota(jnp.int32, (2, 128), 1)
    offset = jnp.zeros((1, 1), F32)
    head = x // 2
    for b in range(NX):
        level = dec[b]
        for k in (1, 2, 4, 8, 16, 32, 64):
            level = level + jnp.where(lane8 >= k, pltpu.roll(level, k, 1), 0.0)
        row = jnp.where(head == 0, level[0:1, :], level[1:2, :]) + offset
        offset = row[:, 127:128]
        grow[:, b * 128 : b * 128 + 128] = row
        gcol[b * 128 : b * 128 + 128, :] = jnp.broadcast_to(row, (128, 128)).T
    dz[z] = jnp.broadcast_to(offset, (8, 128))

    phase("oz_near_far")
    out_z[0].far()
    out_x[0].own()
    out_z[1].near()
    phase("w1")
    ring1.near()
    ring2.own()
    phase("oz_far_far")
    out_z[1].far()
    out_x[1].own()

    def kv_step(step):
        for piece in (0, 1):
            for way in (0, 1):
                kv_arrived(step, way, piece)
                if step < 2 or (step == 2 and piece == way):
                    kv_send(step + 1, way, piece)

    phase("w1_far")
    ring1.far()
    phase("project1")
    project(1)
    phase("q_post")
    qgain = jnp.concatenate([qgain_in[x][0:1, :], qgain_in[x][1:2, :]], axis=1)
    for i in range(NX):
        r = slice(i * 128, i * 128 + 128)
        a = block_rows(i)
        u = map_norm(proj[r, 0:128], qgain)
        u = rope(u, cosd[a, :], sind[a, :], 32).astype(BF16).astype(F32) * 0.125
        u = u.T
        s = slice((i % 2) * 128, (i % 2) * 128 + 128)
        qbd[i // 2, :, s] = jnp.where(sub < 64, u, 0.0).astype(BF16)
        qbd[2 + i // 2, :, s] = jnp.where(sub < 64, 0.0, u).astype(BF16)
        rq[a, :] = rope(proj[r, 128:256], cosr[a, :], sinr[a, :], 64).astype(BF16)

    m_run[...] = jnp.full((4, 1, 256), -jnp.inf, F32)
    l_run[...] = jnp.zeros((4, 1, 256), F32)
    acc[...] = jnp.zeros((4, 128, 256), F32)

    def attend(*origins):
        for q in range(4):
            s = [jnp.dot(kb[o], qbd[q], preferred_element_type=F32) for o in origins]
            before = m_run[q]
            now = before
            for part_s in s:
                now = jnp.maximum(now, jnp.max(part_s, axis=0, keepdims=True))
            shrink = jnp.exp(before - now)
            m_run[q] = now
            total = l_run[q] * shrink
            value = acc[q] * shrink
            for o, part_s in zip(origins, s):
                e = jnp.exp(part_s - now)
                total = total + jnp.sum(e, axis=0, keepdims=True)
                value = value + jnp.dot(vb[o], e.astype(BF16), preferred_element_type=F32)
            l_run[q] = total
            acc[q] = value

    phase("kv_step0")
    kv_step(0)
    phase("attend0")
    attend(z)
    phase("w2")
    ring2.near()
    ring3.own()
    phase("attend1")
    attend(at_z(-1), at_z(1))
    phase("kv_step1")
    kv_step(1)
    phase("attend2")
    attend(at_z(-2), at_z(2))
    phase("ox_near")
    out_x[0].near()
    phase("w2_far")
    ring2.far()
    phase("project2")
    project(2)
    phase("states")
    for i in range(NX):
        r = slice(i * 128, i * 128 + 128)
        a = block_rows(i)
        u = rope(proj[r, 0:128], cosr[a, :], sinr[a, :], 64) * (128 ** -0.5)
        rk[a, :] = u.astype(BF16)
        rv[a, :] = proj[r, 128:256].astype(BF16)
    end = dz[z][0:1, :]
    forward_state = jnp.zeros((128, 128), F32)
    backward_state = jnp.zeros((128, 128), F32)
    for i in range(NX):
        r = slice(i * 128, i * 128 + 128)
        key = rk[r, :].astype(F32)
        value = rv[r, :]
        level = gcol[r, :]
        a = (key * jnp.exp(end - level)).T.astype(BF16)
        b = (key * jnp.exp(level)).T.astype(BF16)
        forward_state += jnp.dot(a, value, preferred_element_type=F32)
        backward_state += jnp.dot(b, value, preferred_element_type=F32)
    st[z, 0] = forward_state.astype(BF16)
    st[z, 1] = backward_state.astype(BF16)

    def st_send(step, way):
        origin = at_z(-step if way == 0 else step)
        device = along_z(zr if way == 0 else zl)
        base = ST + 4 * step + 2 * way
        states = st.at[origin] if step < 3 else st.at[origin, way]
        send(base, states, states, device)
        if step < 3 or way == 1:
            send(base + 1, dz.at[origin], dz.at[origin], device)

    def st_step(step):
        for way in (0, 1):
            origin = at_z(-(step + 1) if way == 0 else step + 1)
            base = ST + 4 * step + 2 * way
            arrived(base, st.at[origin] if step < 3 else st.at[origin, way])
            if step < 3 or way == 1:
                arrived(base + 1, dz.at[origin])
            if step < 3:
                st_send(step + 1, way)

    st_send(0, 0)
    st_send(0, 1)

    phase("w3")
    ring3.near()
    phase("kv_step2")
    kv_step(2)
    phase("attend3")
    attend(at_z(-3), at_z(3))
    phase("st_step0")
    st_step(0)
    phase("ox_far")
    out_x[1].near()
    phase("intra")
    for i in range(NX):
        r = slice(i * 128, i * 128 + 128)
        s = lax.dot_general(rq[r, :], rk[...], (((1,), (1,)), ((), ())), preferred_element_type=F32)
        level = jnp.concatenate([gcol[r, :]] * 4, axis=1)
        w = (s * jnp.exp(-jnp.abs(level - grow[...]))).astype(BF16)
        mix[i] = jnp.dot(w, rv[...], preferred_element_type=F32)

    phase("st_step1")
    st_step(1)
    phase("w3_far")
    ring3.far()
    phase("gate")
    project(3)
    for i in range(NX):
        gate[i] = proj[i * 128 : i * 128 + 128, 0:128].astype(BF16)
    for d, j in ((1, 2), (2, 3), (3, 1)):
        send(GT + d - 1, gate.at[j], gt.at[x], along_x(xs[d]))
    gt[x] = gate[0]

    phase("st_step2")
    st_step(2)
    phase("kv_last")
    kv_arrived(3, 0, 0)
    kv_arrived(3, 1, 1)
    phase("attend4")
    attend(at_z(4))
    phase("diff_out")

    lane4 = lax.broadcasted_iota(jnp.int32, (1, 4), 1)
    lam = jnp.sum(jnp.where(lane4 == x, lam_in[...], 0.0), axis=-1, keepdims=True)
    dgain = dgain_in[pl.ds(x, 1), :]
    for t in range(2):
        first = acc[t] / l_run[t]
        second = acc[2 + t] / l_run[2 + t]
        both = first - lam * second
        both = both * lax.rsqrt(jnp.mean(both * both, axis=0, keepdims=True) + EPS)
        for h in range(2):
            feat[2 * t + h] = (both[:, h * 128 : h * 128 + 128].T * dgain).astype(BF16)
    for d, j in ((1, 2), (2, 3), (3, 1)):
        send(DF + d - 1, feat.at[j], df.at[x], along_x(xs[d]))
    df[x] = feat[0]

    phase("st_step3")
    st_step(3)
    phase("carried")
    forward_state = jnp.zeros((128, 128), F32)
    total = jnp.zeros((1, 128), F32)
    for k in range(NZ - 1, -1, -1):
        take = jnp.where(k < z, 1.0, 0.0)
        forward_state += (jnp.exp(total) * take) * st[k, 0].astype(F32)
        total += dz[k][0:1, :] * take
    backward_state = jnp.zeros((128, 128), F32)
    total = jnp.zeros((1, 128), F32)
    for k in range(NZ):
        take = jnp.where(k > z, 1.0, 0.0)
        backward_state += (jnp.exp(total) * take) * st[k, 1].astype(F32)
        total += dz[k][0:1, :] * take
    states = jnp.concatenate([forward_state, backward_state], axis=0).astype(BF16)
    for i in range(NX):
        r = slice(i * 128, i * 128 + 128)
        query = rq[r, :].astype(F32)
        level = gcol[r, :]
        q2 = jnp.concatenate(
            [(query * jnp.exp(level)).astype(BF16), (query * jnp.exp(end - level)).astype(BF16)],
            axis=1,
        )
        mix[i] = mix[i] + jnp.dot(q2, states, preferred_element_type=F32)
    for d in (1, 2, 3):
        send(RM + d - 1, mix.at[xs[d]], rm.at[x], along_x(xs[d]))
    rm[x] = mix[x]

    phase("o2_far")
    for ring in out_x:
        ring.far()
    phase("home_wait")
    for d in (1, 2, 3):
        arrived(GT + d - 1, gt.at[xs[4 - d]])
        arrived(DF + d - 1, df.at[xs[4 - d]])
        arrived(RM + d - 1, rm.at[xs[4 - d]])
    phase("home")
    for h in range(2):
        a, b = rm[2 * h], rm[2 * h + 1]
        total = jnp.sum(a * a, axis=-1, keepdims=True) + jnp.sum(b * b, axis=-1, keepdims=True)
        scale = lax.rsqrt(total / 256 + EPS)
        for k, m in ((2 * h, a), (2 * h + 1, b)):
            g = gt[k].astype(F32)
            value = (g * jax.nn.sigmoid(g)) * (m * scale * rgain_in[k : k + 1, :])
            fall[:, k * 256 : k * 256 + 128] = value.astype(BF16)
            fall[:, k * 256 + 128 : k * 256 + 256] = df[k]

    phase("out_dot")
    mine = pl.ds(pl.multiple_of(c * 64, 64), 64)
    theirs = pl.ds(pl.multiple_of(other * 64, 64), 64)
    for k in range(NY):
        w = wo[k].reshape(1024, 512)
        part[k] = jnp.dot(fall[...], w, preferred_element_type=F32).astype(BF16)
        send(OUT + k, part.at[k, theirs], pin.at[k], partner)
    phase("out_wait")
    for k in range(NY):
        arrived(OUT + k, pin.at[k])
        value = part[k, mine, :].astype(F32) + pin[k].astype(F32)
        out[0, :, rows_of(ys[(0, 1, 3, 2)[k]] * 512, 512)] = value.astype(BF16)
    phase("drain")
    for copy in sent:
        copy.wait_send()
    phase(None)


def body(
    tokens, norm_gain, retain_query, retain_key, retain_value, retain_gate, differ_query,
    differ_key, differ_value, log_decay, lambdas, query_gain, key_gain, retain_gain,
    differ_gain, retain_out, differ_out,
):
    hbm = pl.BlockSpec(memory_space=pltpu.HBM)
    vmem = pl.BlockSpec(memory_space=pltpu.VMEM)
    V = pltpu.VMEM
    return pl.pallas_call(
        kernel,
        out_shape=jax.ShapeDtypeStruct((1, 64, D), BF16),
        in_specs=[hbm] * 18,
        out_specs=vmem,
        scratch_shapes=[
            V((2, 128), F32), V((1, 4), F32), V((4, 2, 64), F32), V((4, 2, 64), F32),
            V((4, 128), F32), V((4, 128), F32), V((1, D), F32), V((4, 64, 128), F32),
            V((NX, 2, 128, 1024), BF16),
            V((BLOCK, D), BF16),
            V((D, 256), BF16), V((D, 256), BF16), V((D, 256), BF16), V((D, 128), BF16),
            V((NY, NX, 256, 512), BF16),
            V((NX, 2, 128), F32),
            V((NZ, BLOCK, 128), BF16),
            V((NZ, 128, BLOCK), BF16),
            V((NZ, 2, 128, 128), BF16),
            V((NZ, 8, 128), F32),
            V((BLOCK, 128), F32), V((BLOCK, 128), F32), V((BLOCK, 128), F32), V((BLOCK, 128), F32),
            V((BLOCK, 256), F32),
            V((4, 128, 256), BF16),
            V((4, 1, 256), F32), V((4, 1, 256), F32), V((4, 128, 256), F32),
            V((BLOCK, 128), BF16), V((BLOCK, 128), BF16), V((BLOCK, 128), BF16),
            V((1, BLOCK), F32), V((BLOCK, 128), F32),
            V((NX, 128, 128), F32),
            V((NX, 128, 128), BF16), V((NX, 128, 128), BF16),
            V((NX, 128, 128), BF16), V((NX, 128, 128), BF16), V((NX, 128, 128), F32),
            V((128, 1024), BF16),
            V((NY, 128, 512), BF16), V((NY, 64, 512), BF16),
            pltpu.SemaphoreType.DMA((COPIES,)),
            pltpu.SemaphoreType.DMA((COPIES,)),
            pltpu.SemaphoreType.DMA((LOCALS,)),
        ],
        compiler_params=pltpu.CompilerParams(
            collective_id=0, has_side_effects=True, vmem_limit_bytes=67000000
        ),
    )(
        tokens, retain_query, retain_key, retain_value, retain_gate, differ_query, differ_key,
        differ_value, retain_out, differ_out, log_decay[0].T, lambdas.reshape(1, 4), query_gain,
        key_gain, retain_gain.reshape(4, 128), differ_gain.reshape(4, 128), norm_gain.reshape(1, D),
        jnp.asarray(rope_tables()),
    )


def solution(mesh):
    in_specs = (
        P("fs", "sp", "tp"), P(),
        P("fs", "tp"), P("fs", "tp"), P("fs", "tp"), P("fs", "tp"), P("fs", "tp"), P("fs", "tp"), P("fs", "tp"),
        P("fs", "sp", "tp"),
        P("tp"), P("tp", None, None), P("tp", None, None), P("tp"), P("tp"),
        P("tp", "fs"), P("tp", "fs"),
    )
    out_specs = P("fs", ("sp", "tp"), None)
    return jax.shard_map(body, mesh=mesh, in_specs=in_specs, out_specs=out_specs, check_vma=False)
```

```python
import functools

import numpy as np
import jax
import jax.numpy as jnp
from jax import lax
from jax.experimental import pallas as pl
from jax.experimental.pallas import tpu as pltpu
from jax.sharding import PartitionSpec as P

F32 = jnp.float32
BF16 = jnp.bfloat16
MESH = pl.DeviceIdType.MESH
EPS = 1e-06
ROPE_BASE = 10000.0
NX, NY, NZ = 4, 4, 8
ROWS = 128
BLOCK = NX * ROWS
D = 2048
WIDTHS = (256, 256, 128, 256)

TOK = 0
PART = 8
W0 = 16
W1 = 24
W2 = 28
W3 = 32
OY = 36
OZ = 40
OX = 48
DEC = 56
KV = 59
ST = 75
DF = 91
GT = 94
RM = 97
OUT = 100
COPIES = 104
LOCALS = 24


def rope_tables():
    lane = np.arange(128)
    value = np.arange(64, dtype=np.float64)[:, None]
    tables = []
    for group in (32, 64):
        inverse = ROPE_BASE ** (-2.0 * ((lane % group) % (group // 2)) / group)
        angle = value * inverse[None, :]
        sign = np.where((lane % group) < group // 2, -1.0, 1.0)[None, :]
        tables += [np.cos(angle), np.sin(angle) * sign]
    return np.stack(tables).astype(np.float32)


class Phases:
    def __init__(self):
        self.scope = None

    def __call__(self, name):
        if self.scope is not None:
            self.scope.__exit__(None, None, None)
        self.scope = jax.named_scope(name) if name else None
        if self.scope is not None:
            self.scope.__enter__()


def kernel(
    tok_in, w_rq, w_rk, w_rv, w_rg, w_dq, w_dk, w_dv, w_ro, w_do,
    dec_hbm, lam_hbm, qgain_hbm, kgain_hbm, rgain_hbm, dgain_hbm, ngain_hbm, tab_hbm,
    out,
    dec_in, lam_in, qgain_in, kgain_in, rgain_in, dgain_in, gain_in, tab, tok, xn, wg0, wg1, wg2, wg3, wo, dec, kb, vb, st, dz, cosd, sind, cosr, sinr, proj, proj2, qbd,
    m_run, l_run, acc, rq, rk, rv, grow, gcol, mix, gate, feat, df, gt, rm, fall, part, pin, mixed, total_out,
    ssem, rsem, lsem,
):
    phase = Phases()
    sp = lax.axis_index("sp")
    z, x = sp // NX, sp % NX
    y = lax.axis_index("fs")
    c = lax.axis_index("tp")
    other = 1 - c

    def along_x(i):
        return {"sp": z * NX + i}

    def along_y(i):
        return {"fs": i}

    def along_z(i):
        return {"sp": i * NX + x}

    partner = {"tp": other}
    xs = [x, (x + 1) % NX, (x + 2) % NX, (x + 3) % NX]
    ys = [y, (y + 1) % NY, (y + 2) % NY, (y + 3) % NY]
    zr, zl = (z + 1) % NZ, (z + NZ - 1) % NZ

    def remote(i, src, dst, device):
        return pltpu.make_async_remote_copy(
            src_ref=src, dst_ref=dst, send_sem=ssem.at[i], recv_sem=rsem.at[i],
            device_id=device, device_id_type=MESH,
        )

    sent = []

    def send(i, src, dst, device):
        copy = remote(i, src, dst, device)
        copy.start()
        sent.append(copy)

    def arrived(i, ref):
        remote(i, ref, ref, partner).wait_recv()

    class Ring4:
        def __init__(self, base, right, left, own, to_right, to_left, half, onward, far):
            self.base, self.right, self.left = base, right, left
            self.src, self.to_right, self.to_left, self.half = own, to_right, to_left, half
            self.onward, self.far_half = onward, far

        def own(self):
            send(self.base, self.src, self.to_right, self.right)
            send(self.base + 1, self.src, self.to_left, self.left)

        def wait(self):
            arrived(self.base, self.half[2])
            arrived(self.base + 1, self.half[3])

        def forward(self):
            send(self.base + 2, self.half[0], self.onward[0], self.right)
            send(self.base + 3, self.half[1], self.onward[1], self.left)

        def near(self):
            self.wait()
            self.forward()

        def far(self):
            arrived(self.base + 2, self.far_half[0])
            arrived(self.base + 3, self.far_half[1])

    def ring_at(base, at, sides, full, half):
        return Ring4(
            base, sides[0], sides[1], full(at[0]), full(at[0]), full(at[0]),
            (half(at[3], 0), half(at[1], 1), full(at[3]), full(at[1])),
            (half(at[3], 0), half(at[1], 1)), (half(at[2], 0), half(at[2], 1)),
        )

    wgs = (wg0, wg1, wg2, wg3)
    def rows_of(start, size):
        return pl.ds(pl.multiple_of(start, size & -size), size)

    token_rings = [
        ring_at(
            TOK + 4 * piece, xs, (along_x(xs[1]), along_x(xs[3])),
            lambda i, p=piece: tok.at[i, c, pl.ds(p * 64, 64)],
            lambda i, h, p=piece: tok.at[i, c, pl.ds(p * 64 + h * 32, 32)],
        )
        for piece in (0, 1)
    ]

    def weight_ring(base, ref, start, size):
        return ring_at(
            base, ys, (along_y(ys[1]), along_y(ys[3])),
            lambda i: ref.at[rows_of(i * 512 + start, size)],
            lambda i, h: ref.at[rows_of(i * 512 + start + h * (size // 2), size // 2)],
        )

    ring0 = [weight_ring(W0 + 4 * piece, wg0, piece * 256, 256) for piece in (0, 1)]
    ring1 = weight_ring(W1, wg1, 0, 512)
    ring2 = weight_ring(W2, wg2, 0, 512)
    ring3 = weight_ring(W3, wg3, 0, 512)

    zc = z % 4
    zcs = [(zc + d) % 4 for d in range(4)]

    def slice_of(slot, i, h=None):
        if h is None:
            return wo.at[slot, x, rows_of(i * 64, 64)]
        return wo.at[slot, x, rows_of(i * 64 + h * 32, 32)]

    out_y = Ring4(
        OY, along_y(ys[1]), along_y(ys[3]), slice_of(0, zc), slice_of(2, zc), slice_of(1, zc),
        (slice_of(2, zc, 0), slice_of(1, zc, 1), slice_of(2, zc), slice_of(1, zc)),
        (slice_of(3, zc, 0), slice_of(3, zc, 1)), (slice_of(3, zc, 0), slice_of(3, zc, 1)),
    )

    near, far = pl.ds(1, 2), 3
    out_z = []
    out_x = []
    for k, slot in enumerate((near, far)):
        piece = functools.partial(slice_of, slot)
        out_z.append(ring_at(OZ + 4 * k, zcs, (along_z(zr), along_z(zl)), piece, piece))
        out_x.append(
            ring_at(
                OX + 4 * k, xs, (along_x(xs[1]), along_x(xs[3])),
                lambda i, s=slot: wo.at[s, i],
                lambda i, h, s=slot: wo.at[s, i, pl.ds(h * 128, 128)],
            )
        )

    def local(i, src, dst):
        copy = pltpu.make_async_copy(src, dst, lsem.at[i])
        copy.start()
        return copy

    col = pl.ds(pl.multiple_of(x * 128, 128), 128)
    col2 = pl.ds(pl.multiple_of((x // 2) * 128, 128), 128)
    own_rows = pl.ds(pl.multiple_of(y * 512, 512), 512)
    lo, hi = pl.ds(0, 128), pl.ds(128, 128)
    load_tok = local(0, tok_in.at[0], tok.at[x, c])
    load_g = [
        [local(1, w_dk.at[:, col], wg0.at[own_rows, lo]), local(2, w_dv.at[:, col], wg0.at[own_rows, hi])],
        [local(3, w_rk.at[:, col2], wg1.at[own_rows, lo]), local(4, w_rv.at[:, col], wg1.at[own_rows, hi])],
        [local(5, w_dq.at[:, col], wg2.at[own_rows])],
        [local(6, w_rq.at[:, col2], wg3.at[own_rows, lo]), local(7, w_rg.at[:, col], wg3.at[own_rows, hi])],
    ]
    load_o = []
    for i in range(NX):
        src = (w_ro, w_do)[i // 2]
        load_o.append(local(8 + i, src.at[pl.ds((i % 2) * 256, 256)], wo.at[0, i]))

    load_small = [
        local(16 + i, src, dst)
        for i, (src, dst) in enumerate((
            (dec_hbm, dec_in), (lam_hbm, lam_in), (qgain_hbm, qgain_in), (kgain_hbm, kgain_in),
            (rgain_hbm, rgain_in), (dgain_hbm, dgain_in), (ngain_hbm, gain_in), (tab_hbm, tab),
        ))
    ]

    phase("barrier")
    barrier = pltpu.get_barrier_semaphore()
    peers = [along_x(xs[1]), along_x(xs[2]), along_x(xs[3]), along_y(ys[1]), along_y(ys[3]),
             along_z(zr), along_z(zl), partner]
    for peer in peers:
        pl.semaphore_signal(barrier, inc=1, device_id=peer, device_id_type=MESH)
    pl.semaphore_wait(barrier, len(peers))

    phase("loads")
    for copy in load_o:
        copy.wait()
    out_y.own()
    load_tok.wait()
    for ring in token_rings:
        ring.own()
    send(PART, tok.at[x, c], tok.at[x, c], partner)
    for copy in load_g[0]:
        copy.wait()
    for ring in ring0:
        ring.own()
    for copy in load_small:
        copy.wait()
    for d in (1, 2, 3):
        send(DEC + d - 1, dec_in, dec.at[x], along_x(xs[d]))
    dec[x] = dec_in[...]
    for group in load_g[1:]:
        for copy in group:
            copy.wait()

    lane = lax.broadcasted_iota(jnp.int32, (128, 128), 1)
    sub = lax.broadcasted_iota(jnp.int32, (128, 128), 0)

    phase("tables")
    lane64 = lax.broadcasted_iota(jnp.int32, (64, 128), 1)
    zrow = pl.ds(pl.multiple_of(z * 8, 8), 8)
    for k, ref in enumerate((cosd, sind, cosr, sinr)):
        by_row = tab[k, zrow, :]
        by_col = tab[k]
        is_row = (lane64 % 64) < 32 if k < 2 else lane64 < 64
        for b in range(8):
            ref[b * 64 : b * 64 + 64, :] = jnp.where(is_row, by_row[b : b + 1, :], by_col)

    def rope(u, cos, sin, group):
        half = group // 2
        up = pltpu.roll(u, 128 - half, 1)
        down = pltpu.roll(u, half, 1)
        return u * cos + jnp.where((lane % group) < half, up, down) * sin

    def map_norm(u, gain):
        square = u * u
        first = jnp.sum(jnp.where(lane < 64, square, 0.0), axis=-1, keepdims=True)
        second = jnp.sum(jnp.where(lane < 64, 0.0, square), axis=-1, keepdims=True)
        scale = jnp.where(
            lane < 64, lax.rsqrt(first / 64 + EPS), lax.rsqrt(second / 64 + EPS)
        )
        return u * scale * gain

    order = [xs[0], xs[3], xs[1], xs[2]]

    def block_rows(j):
        return rows_of(order[j] * 128, 128)

    def normalize(j):
        i = order[j]
        for k in range(8):
            r = slice(k * 16, k * 16 + 16)
            w = slice(j * 128 + k * 16, j * 128 + k * 16 + 16)
            a = tok[i, 0, r, :].astype(F32)
            b = tok[i, 1, r, :].astype(F32)
            total = jnp.sum(a * a, axis=-1, keepdims=True) + jnp.sum(b * b, axis=-1, keepdims=True)
            scale = lax.rsqrt(total / D + EPS)
            xn[w, 0:1024] = (a * scale * gain_in[:, 0:1024]).astype(BF16)
            xn[w, 1024:2048] = (b * scale * gain_in[:, 1024:2048]).astype(BF16)

    def project(g, start=0, size=BLOCK):
        ref = wgs[g]
        width = WIDTHS[g]
        step = 256 if size % 256 == 0 else 128
        for j in range(start, start + size, step):
            proj[j : j + step, 0:width] = jnp.dot(
                xn[j : j + step, :], ref[...], preferred_element_type=F32
            )

    def part_send(n, block, start, size):
        ref = tok.at[block, c, pl.ds(start, size)]
        send(PART + n, ref, ref, partner)

    def part_arrived(n, block, start, size):
        arrived(PART + n, tok.at[block, other, pl.ds(start, size)])

    kgain = jnp.concatenate([kgain_in[x][0:1, :], kgain_in[x][1:2, :]], axis=1)

    def keys_values(j):
        r = slice(j * 128, j * 128 + 128)
        a = block_rows(j)
        u = map_norm(proj[r, 0:128], kgain)
        kb[z, r, :] = rope(u, cosd[a, :], sind[a, :], 32).astype(BF16)
        vb[z, :, r] = proj[r, 128:256].T.astype(BF16)

    phase("oy")
    out_y.near()
    out_z[0].own()
    phase("tok_a")
    token_rings[0].near()
    part_send(1, order[1], 0, 64)
    part_send(2, order[2], 0, 64)
    phase("w0a")
    ring0[0].near()
    phase("tok_b")
    token_rings[1].near()
    part_send(3, order[1], 64, 64)
    part_send(4, order[2], 64, 64)
    phase("oy_far")
    out_y.far()
    out_z[1].own()
    phase("oz_near")
    out_z[0].near()
    phase("norm0")
    arrived(PART, tok.at[x, other])
    normalize(0)
    phase("w0b")
    ring0[1].near()
    ring1.own()
    ring2.own()
    phase("tok_far_a")
    token_rings[0].far()
    part_send(5, order[3], 0, 64)
    phase("norm12")
    for j in (1, 2):
        part_arrived(j, order[j], 0, 64)
        part_arrived(2 + j, order[j], 64, 64)
        normalize(j)
    phase("tok_far_b")
    token_rings[1].far()
    part_send(6, order[3], 64, 64)
    phase("oz_far_near")
    out_z[1].near()
    phase("norm3")
    part_arrived(5, order[3], 0, 64)
    part_arrived(6, order[3], 64, 64)
    normalize(3)
    phase("w0_far")
    for ring in ring0:
        ring.far()
    phase("project0")
    project(0)
    phase("kv_post")
    for j in range(4):
        keys_values(j)

    zs = [(z + NZ + d) % NZ for d in range(-4, 5)]

    def at_z(d):
        return zs[d + 4]

    def kv_send(step, way, piece):
        origin = at_z(-step if way == 0 else step)
        ref = (kb, vb)[piece].at[origin]
        send(KV + 4 * step + 2 * way + piece, ref, ref, along_z(zr if way == 0 else zl))

    def kv_arrived(step, way, piece):
        origin = at_z(-(step + 1) if way == 0 else step + 1)
        arrived(KV + 4 * step + 2 * way + piece, (kb, vb)[piece].at[origin])

    for piece in (0, 1):
        for way in (0, 1):
            kv_send(0, way, piece)

    phase("levels")
    phase("oz_near_far")
    out_z[0].far()
    out_x[0].own()
    phase("levels")
    for d in (1, 2, 3):
        arrived(DEC + d - 1, dec.at[xs[4 - d]])
    lane8 = lax.broadcasted_iota(jnp.int32, (2, 128), 1)
    offset = jnp.zeros((1, 1), F32)
    head = x // 2
    for b in range(NX):
        level = dec[b]
        for k in (1, 2, 4, 8, 16, 32, 64):
            level = level + jnp.where(lane8 >= k, pltpu.roll(level, k, 1), 0.0)
        row = jnp.where(head == 0, level[0:1, :], level[1:2, :]) + offset
        offset = row[:, 127:128]
        grow[:, b * 128 : b * 128 + 128] = row
        gcol[b * 128 : b * 128 + 128, :] = jnp.broadcast_to(row, (128, 128)).T
    dz[z] = jnp.broadcast_to(offset, (8, 128))

    def kv_step(step, piece):
        for way in (0, 1):
            kv_arrived(step, way, piece)
            if step < 2 or (step == 2 and piece == way):
                kv_send(step + 1, way, piece)

    phase("w1")
    ring1.near()
    phase("k0")
    kv_step(0, 0)
    phase("w2")
    ring2.near()
    ring3.own()
    phase("v0")
    kv_step(0, 1)
    phase("w1_far")
    ring1.far()
    phase("project1")
    project(1)
    phase("states")
    for i in range(NX):
        r = slice(i * 128, i * 128 + 128)
        a = block_rows(i)
        u = rope(proj[r, 0:128], cosr[a, :], sinr[a, :], 64) * (128 ** -0.5)
        rk[a, :] = u.astype(BF16)
        rv[a, :] = proj[r, 128:256].astype(BF16)
    end = dz[z][0:1, :]
    forward_state = jnp.zeros((128, 128), F32)
    backward_state = jnp.zeros((128, 128), F32)
    for i in range(NX):
        r = slice(i * 128, i * 128 + 128)
        key = rk[r, :].astype(F32)
        value = rv[r, :]
        level = gcol[r, :]
        a = (key * jnp.exp(end - level)).T.astype(BF16)
        b = (key * jnp.exp(level)).T.astype(BF16)
        forward_state += jnp.dot(a, value, preferred_element_type=F32)
        backward_state += jnp.dot(b, value, preferred_element_type=F32)
    st[z, 0] = forward_state.astype(BF16)
    st[z, 1] = backward_state.astype(BF16)

    def st_send(step, way):
        origin = at_z(-step if way == 0 else step)
        device = along_z(zr if way == 0 else zl)
        base = ST + 4 * step + 2 * way
        states = st.at[origin] if step < 3 else st.at[origin, way]
        send(base, states, states, device)
        if step < 3 or way == 1:
            send(base + 1, dz.at[origin], dz.at[origin], device)

    def st_step(step):
        for way in (0, 1):
            origin = at_z(-(step + 1) if way == 0 else step + 1)
            base = ST + 4 * step + 2 * way
            arrived(base, st.at[origin] if step < 3 else st.at[origin, way])
            if step < 3 or way == 1:
                arrived(base + 1, dz.at[origin])
            if step < 3:
                st_send(step + 1, way)

    st_send(0, 0)
    st_send(0, 1)

    m_run[...] = jnp.full((4, 1, 256), -jnp.inf, F32)
    l_run[...] = jnp.zeros((4, 1, 256), F32)
    acc[...] = jnp.zeros((4, 128, 256), F32)

    def attend(origins, tiles):
        for q in tiles:
            s = [jnp.dot(kb[o], qbd[q], preferred_element_type=F32) for o in origins]
            before = m_run[q]
            now = before
            for part_s in s:
                now = jnp.maximum(now, jnp.max(part_s, axis=0, keepdims=True))
            shrink = jnp.exp(before - now)
            m_run[q] = now
            total = l_run[q] * shrink
            value = acc[q] * shrink
            for o, part_s in zip(origins, s):
                e = jnp.exp(part_s - now)
                total = total + jnp.sum(e, axis=0, keepdims=True)
                value = value + jnp.dot(vb[o], e.astype(BF16), preferred_element_type=F32)
            l_run[q] = total
            acc[q] = value

    phase("w2_far")
    ring2.far()
    phase("k1")
    kv_step(1, 0)
    phase("project2")
    project(2)
    phase("q_post")
    query_order = [3, 1, 2, 0]
    qgain = jnp.concatenate([qgain_in[x][0:1, :], qgain_in[x][1:2, :]], axis=1)
    for p, i in enumerate(query_order):
        r = slice(i * 128, i * 128 + 128)
        a = block_rows(i)
        u = map_norm(proj[r, 0:128], qgain)
        u = rope(u, cosd[a, :], sind[a, :], 32).astype(BF16).astype(F32) * 0.125
        u = u.T
        s = slice((p % 2) * 128, (p % 2) * 128 + 128)
        qbd[p // 2, :, s] = jnp.where(sub < 64, u, 0.0).astype(BF16)
        qbd[2 + p // 2, :, s] = jnp.where(sub < 64, 0.0, u).astype(BF16)

    phase("v1")
    kv_step(1, 1)
    phase("attend0a")
    attend((z,), (0, 1))
    phase("oz_far_far")
    out_z[1].far()
    out_x[1].own()
    phase("st_step0")
    st_step(0)
    phase("attend0b")
    attend((z,), (2, 3))
    phase("ox_near")
    out_x[0].near()
    phase("attend1a")
    attend((at_z(-1), at_z(1)), (0, 1))
    phase("k2")
    kv_step(2, 0)
    phase("attend1b")
    attend((at_z(-1), at_z(1)), (2, 3))
    phase("w3")
    ring3.near()
    phase("attend2a")
    attend((at_z(-2), at_z(2)), (0, 1))
    phase("v2")
    kv_step(2, 1)
    phase("attend2b")
    attend((at_z(-2), at_z(2)), (2, 3))
    phase("st_step1")
    st_step(1)
    phase("ox_far")
    out_x[1].near()
    phase("w3_far")
    ring3.far()
    phase("project3")
    project(3)
    for i in range(NX):
        r = slice(i * 128, i * 128 + 128)
        a = block_rows(i)
        rq[a, :] = rope(proj[r, 0:128], cosr[a, :], sinr[a, :], 64).astype(BF16)
        gate[i] = proj[r, 128:256].astype(BF16)
    for d, j in ((1, 2), (2, 3), (3, 1)):
        send(GT + d - 1, gate.at[j], gt.at[x], along_x(xs[d]))
    gt[x] = gate[0]

    phase("intra")
    for i in range(NX):
        r = slice(i * 128, i * 128 + 128)
        s = lax.dot_general(rq[r, :], rk[...], (((1,), (1,)), ((), ())), preferred_element_type=F32)
        level = jnp.concatenate([gcol[r, :]] * 4, axis=1)
        w = (s * jnp.exp(-jnp.abs(level - grow[...]))).astype(BF16)
        mix[i] = jnp.dot(w, rv[...], preferred_element_type=F32)

    phase("attend3a")
    attend((at_z(-3), at_z(3)), (0, 2))
    phase("st_step2")
    st_step(2)
    phase("attend3b")
    attend((at_z(-3), at_z(3)), (1, 3))
    phase("kv_last")
    kv_arrived(3, 0, 0)
    kv_arrived(3, 1, 1)

    lane4 = lax.broadcasted_iota(jnp.int32, (1, 4), 1)
    lam = jnp.sum(jnp.where(lane4 == x, lam_in[...], 0.0), axis=-1, keepdims=True)
    dgain = dgain_in[pl.ds(x, 1), :]

    def differ_out(t):
        first = acc[t] / l_run[t]
        second = acc[2 + t] / l_run[2 + t]
        both = first - lam * second
        both = both * lax.rsqrt(jnp.mean(both * both, axis=0, keepdims=True) + EPS)
        for h in range(2):
            j = query_order[2 * t + h]
            feat[j] = (both[:, h * 128 : h * 128 + 128].T * dgain).astype(BF16)

    phase("attend4a")
    attend((at_z(4),), (0, 2))
    phase("differ_out_a")
    differ_out(0)
    send(DF + 1, feat.at[3], df.at[x], along_x(xs[2]))
    send(DF + 2, feat.at[1], df.at[x], along_x(xs[3]))
    phase("st_step3")
    st_step(3)
    phase("carried")
    forward_state = jnp.zeros((128, 128), F32)
    total = jnp.zeros((1, 128), F32)
    for k in range(NZ - 1, -1, -1):
        take = jnp.where(k < z, 1.0, 0.0)
        forward_state += (jnp.exp(total) * take) * st[k, 0].astype(F32)
        total += dz[k][0:1, :] * take
    backward_state = jnp.zeros((128, 128), F32)
    total = jnp.zeros((1, 128), F32)
    for k in range(NZ):
        take = jnp.where(k > z, 1.0, 0.0)
        backward_state += (jnp.exp(total) * take) * st[k, 1].astype(F32)
        total += dz[k][0:1, :] * take
    states = jnp.concatenate([forward_state, backward_state], axis=0).astype(BF16)
    for i in range(NX):
        r = slice(i * 128, i * 128 + 128)
        query = rq[r, :].astype(F32)
        level = gcol[r, :]
        q2 = jnp.concatenate(
            [(query * jnp.exp(level)).astype(BF16), (query * jnp.exp(end - level)).astype(BF16)],
            axis=1,
        )
        total = mix[i] + jnp.dot(q2, states, preferred_element_type=F32)
        mixed[i] = total.astype(BF16)
    send(RM + 1, mixed.at[xs[2]], rm.at[x], along_x(xs[2]))
    send(RM, mixed.at[xs[1]], rm.at[x], along_x(xs[1]))
    send(RM + 2, mixed.at[xs[3]], rm.at[x], along_x(xs[3]))
    rm[x] = mixed[x]
    phase("attend4b")
    attend((at_z(4),), (1, 3))
    phase("differ_out_b")
    differ_out(1)
    send(DF, feat.at[2], df.at[x], along_x(xs[1]))
    df[x] = feat[0]

    phase("ox_far_far")
    for ring in out_x:
        ring.far()
    phase("home_wait_r")
    for d in (1, 2, 3):
        arrived(GT + d - 1, gt.at[xs[4 - d]])
        arrived(RM + d - 1, rm.at[xs[4 - d]])
    phase("home_r")
    for h in range(2):
        a, b = rm[2 * h].astype(F32), rm[2 * h + 1].astype(F32)
        total = jnp.sum(a * a, axis=-1, keepdims=True) + jnp.sum(b * b, axis=-1, keepdims=True)
        scale = lax.rsqrt(total / 256 + EPS)
        for k, m in ((2 * h, a), (2 * h + 1, b)):
            g = gt[k].astype(F32)
            value = (g * jax.nn.sigmoid(g)) * (m * scale * rgain_in[k : k + 1, :])
            fall[:, k * 128 : k * 128 + 128] = value.astype(BF16)
    for k in range(NY):
        w = wo[k].reshape(1024, 512)[0:512]
        total_out[k] = jnp.dot(fall[:, 0:512], w, preferred_element_type=F32)
    phase("home_wait_d")
    for d in (1, 2, 3):
        arrived(DF + d - 1, df.at[xs[4 - d]])
    for k in range(NX):
        fall[:, 512 + k * 128 : 640 + k * 128] = df[k]
    phase("out_dot")
    mine = pl.ds(pl.multiple_of(c * 64, 64), 64)
    theirs = pl.ds(pl.multiple_of(other * 64, 64), 64)
    for k in range(NY):
        w = wo[k].reshape(1024, 512)[512:1024]
        total = total_out[k] + jnp.dot(fall[:, 512:1024], w, preferred_element_type=F32)
        part[k] = total.astype(BF16)
        send(OUT + k, part.at[k, theirs], pin.at[k], partner)
    phase("out_wait")
    for k in range(NY):
        arrived(OUT + k, pin.at[k])
        value = part[k, mine, :].astype(F32) + pin[k].astype(F32)
        out[0, :, rows_of(ys[(0, 1, 3, 2)[k]] * 512, 512)] = value.astype(BF16)
    phase("drain")
    for copy in sent:
        copy.wait_send()
    phase(None)


def body(
    tokens, norm_gain, retain_query, retain_key, retain_value, retain_gate, differ_query,
    differ_key, differ_value, log_decay, lambdas, query_gain, key_gain, retain_gain,
    differ_gain, retain_out, differ_out,
):
    hbm = pl.BlockSpec(memory_space=pltpu.HBM)
    vmem = pl.BlockSpec(memory_space=pltpu.VMEM)
    V = pltpu.VMEM
    return pl.pallas_call(
        kernel,
        out_shape=jax.ShapeDtypeStruct((1, 64, D), BF16),
        in_specs=[hbm] * 18,
        out_specs=vmem,
        scratch_shapes=[
            V((2, 128), F32), V((1, 4), F32), V((4, 2, 64), F32), V((4, 2, 64), F32),
            V((4, 128), F32), V((4, 128), F32), V((1, D), F32), V((4, 64, 128), F32),
            V((NX, 2, 128, 1024), BF16),
            V((BLOCK, D), BF16),
            V((D, 256), BF16), V((D, 256), BF16), V((D, 128), BF16), V((D, 256), BF16),
            V((NY, NX, 256, 512), BF16),
            V((NX, 2, 128), F32),
            V((NZ, BLOCK, 128), BF16),
            V((NZ, 128, BLOCK), BF16),
            V((NZ, 2, 128, 128), BF16),
            V((NZ, 8, 128), F32),
            V((BLOCK, 128), F32), V((BLOCK, 128), F32), V((BLOCK, 128), F32), V((BLOCK, 128), F32),
            V((BLOCK, 256), F32), V((BLOCK, 128), F32),
            V((4, 128, 256), BF16),
            V((4, 1, 256), F32), V((4, 1, 256), F32), V((4, 128, 256), F32),
            V((BLOCK, 128), BF16), V((BLOCK, 128), BF16), V((BLOCK, 128), BF16),
            V((1, BLOCK), F32), V((BLOCK, 128), F32),
            V((NX, 128, 128), F32),
            V((NX, 128, 128), BF16), V((NX, 128, 128), BF16),
            V((NX, 128, 128), BF16), V((NX, 128, 128), BF16), V((NX, 128, 128), BF16),
            V((128, 1024), BF16),
            V((NY, 128, 512), BF16), V((NY, 64, 512), BF16),
            V((NX, 128, 128), BF16), V((NY, 128, 512), F32),
            pltpu.SemaphoreType.DMA((COPIES,)),
            pltpu.SemaphoreType.DMA((COPIES,)),
            pltpu.SemaphoreType.DMA((LOCALS,)),
        ],
        compiler_params=pltpu.CompilerParams(
            collective_id=0, has_side_effects=True, vmem_limit_bytes=67000000
        ),
    )(
        tokens, retain_query, retain_key, retain_value, retain_gate, differ_query, differ_key,
        differ_value, retain_out, differ_out, log_decay[0].T, lambdas.reshape(1, 4), query_gain,
        key_gain, retain_gain.reshape(4, 128), differ_gain.reshape(4, 128), norm_gain.reshape(1, D),
        jnp.asarray(rope_tables()),
    )


def solution(mesh):
    in_specs = (
        P("fs", "sp", "tp"), P(),
        P("fs", "tp"), P("fs", "tp"), P("fs", "tp"), P("fs", "tp"), P("fs", "tp"), P("fs", "tp"), P("fs", "tp"),
        P("fs", "sp", "tp"),
        P("tp"), P("tp", None, None), P("tp", None, None), P("tp"), P("tp"),
        P("tp", "fs"), P("tp", "fs"),
    )
    out_specs = P("fs", ("sp", "tp"), None)
    return jax.shard_map(body, mesh=mesh, in_specs=in_specs, out_specs=out_specs, check_vma=False)
```

```python
import functools

import numpy as np
import jax
import jax.numpy as jnp
from jax import lax
from jax.experimental import pallas as pl
from jax.experimental.pallas import tpu as pltpu
from jax.sharding import PartitionSpec as P

F32 = jnp.float32
BF16 = jnp.bfloat16
MESH = pl.DeviceIdType.MESH
EPS = 1e-06
ROPE_BASE = 10000.0
NX, NY, NZ = 4, 4, 8
ROWS = 128
BLOCK = NX * ROWS
D = 2048
WIDTHS = (256, 256, 128, 256)

TOK = 0
PART = 8
W0 = 16
W1 = 24
W2 = 28
W3 = 32
OY = 36
OZ = 40
OX = 48
DEC = 56
KV = 59
ST = 75
DF = 91
GT = 94
RM = 97
OUT = 100
COPIES = 104
SENDS = 50
LOCALS = 20


def rope_tables():
    lane = np.arange(128)
    value = np.arange(64, dtype=np.float64)[:, None]
    tables = []
    for group in (32, 64):
        inverse = ROPE_BASE ** (-2.0 * ((lane % group) % (group // 2)) / group)
        angle = value * inverse[None, :]
        sign = np.where((lane % group) < group // 2, -1.0, 1.0)[None, :]
        tables += [np.cos(angle), np.sin(angle) * sign]
    return np.stack(tables).astype(np.float32)


class Phases:
    def __init__(self):
        self.scope = None

    def __call__(self, name):
        if self.scope is not None:
            self.scope.__exit__(None, None, None)
        self.scope = jax.named_scope(name) if name else None
        if self.scope is not None:
            self.scope.__enter__()


def kernel(
    tok_in, w_rq, w_rk, w_rv, w_rg, w_dq, w_dk, w_dv, w_ro, w_do,
    dec_hbm, lam_hbm, qgain_hbm, kgain_hbm, rgain_hbm, dgain_hbm, ngain_hbm, tab_hbm,
    out,
    dec_in, lam_in, qgain_in, kgain_in, rgain_in, dgain_in, gain_in, tab, tok, xn, wg0, wg1, wg2, wg3, wo, dec, kb, vb, st, dz, cosd, sind, cosr, sinr, proj, proj2, qbd,
    m_run, l_run, acc, rq, rk, rv, grow, gcol, mix, gate, feat, df, gt, rm, fall, part, mixed, total_out,
    ssem, rsem, lsem,
):
    phase = Phases()
    sp = lax.axis_index("sp")
    z, x = sp // NX, sp % NX
    y = lax.axis_index("fs")
    c = lax.axis_index("tp")
    other = 1 - c

    def along_x(i):
        return {"sp": z * NX + i}

    def along_y(i):
        return {"fs": i}

    def along_z(i):
        return {"sp": i * NX + x}

    partner = {"tp": other}
    xs = [x, (x + 1) % NX, (x + 2) % NX, (x + 3) % NX]
    ys = [y, (y + 1) % NY, (y + 2) % NY, (y + 3) % NY]
    zr, zl = (z + 1) % NZ, (z + NZ - 1) % NZ

    sent = []
    rings_sent = {}

    def send(i, src, dst, device, ring=None):
        n = len(sent) if ring is None else rings_sent.setdefault(id(ring), (len(sent), ring))[0]
        copy = pltpu.make_async_remote_copy(
            src_ref=src, dst_ref=dst, send_sem=ssem.at[n], recv_sem=rsem.at[i],
            device_id=device, device_id_type=MESH,
        )
        copy.start()
        if n == len(sent):
            sent.append(copy if ring is None else None)

    def arrived(i, ref):
        pltpu.make_async_remote_copy(
            src_ref=ref, dst_ref=ref, send_sem=ssem.at[0], recv_sem=rsem.at[i],
            device_id=partner, device_id_type=MESH,
        ).wait_recv()

    class Ring4:
        def __init__(self, base, right, left, own, to_right, to_left, half, onward, far, three):
            self.base, self.right, self.left = base, right, left
            self.src, self.to_right, self.to_left, self.half = own, to_right, to_left, half
            self.onward, self.far_half = onward, far
            self.three = three

        def own(self):
            send(self.base, self.src, self.to_right, self.right, self.three)
            send(self.base + 1, self.src, self.to_left, self.left, self.three)

        def wait(self):
            arrived(self.base, self.half[2])
            arrived(self.base + 1, self.half[3])

        def forward(self):
            send(self.base + 2, self.half[0], self.onward[0], self.right, self.three)
            send(self.base + 3, self.half[1], self.onward[1], self.left, self.three)

        def near(self):
            self.wait()
            self.forward()

        def far(self):
            arrived(self.base + 2, self.far_half[0])
            arrived(self.base + 3, self.far_half[1])

    def ring_at(base, at, sides, full, half, three):
        return Ring4(
            base, sides[0], sides[1], full(at[0]), full(at[0]), full(at[0]),
            (half(at[3], 0), half(at[1], 1), full(at[3]), full(at[1])),
            (half(at[3], 0), half(at[1], 1)), (half(at[2], 0), half(at[2], 1)), three,
        )

    wgs = (wg0, wg1, wg2, wg3)
    def rows_of(start, size):
        return pl.ds(pl.multiple_of(start, size & -size), size)

    def token_half(i, h):
        return tok.at[i, c, pl.ds(h * 64, 64)]

    six = tok.at[pl.ds(0, 3), 0]

    def token_send(n, i, h, to):
        send(TOK + n, token_half(i, h), token_half(i, h), along_x(xs[to]), six)

    def tokens_own():
        for n, h, to in ((0, 0, 1), (1, 1, 3), (2, 1, 1), (3, 0, 3)):
            token_send(n, xs[0], h, to)

    def tokens_first():
        arrived(TOK, token_half(xs[3], 0))
        token_send(4, xs[3], 0, 1)
        arrived(TOK + 1, token_half(xs[1], 1))
        token_send(5, xs[1], 1, 3)

    def tokens_second():
        arrived(TOK + 2, token_half(xs[3], 1))
        arrived(TOK + 3, token_half(xs[1], 0))

    def weight_ring(base, ref, start, size):
        return ring_at(
            base, ys, (along_y(ys[1]), along_y(ys[3])),
            lambda i: ref.at[rows_of(i * 512 + start, size)],
            lambda i, h: ref.at[rows_of(i * 512 + start + h * (size // 2), size // 2)],
            ref.at[pl.ds(start, 3 * size)],
        )

    def weight_half(i, h):
        return wg0.at[rows_of(i * 512 + h * 256, 256)]

    three_blocks = wg0.at[pl.ds(0, 1536)]

    def weight_send(n, i, h, to):
        send(W0 + n, weight_half(i, h), weight_half(i, h), along_y(ys[to]), three_blocks)

    def weights_own():
        for n, h, to in ((0, 0, 1), (1, 1, 3), (2, 1, 1), (3, 0, 3)):
            weight_send(n, ys[0], h, to)

    def weights_first():
        arrived(W0, weight_half(ys[3], 0))
        weight_send(4, ys[3], 0, 1)
        arrived(W0 + 1, weight_half(ys[1], 1))
        weight_send(5, ys[1], 1, 3)

    def weights_rest():
        arrived(W0 + 2, weight_half(ys[3], 1))
        arrived(W0 + 3, weight_half(ys[1], 0))
        arrived(W0 + 4, weight_half(ys[2], 0))
        arrived(W0 + 5, weight_half(ys[2], 1))

    ring1 = weight_ring(W1, wg1, 0, 512)
    ring2 = weight_ring(W2, wg2, 0, 512)
    ring3 = weight_ring(W3, wg3, 0, 512)

    zc = z % 4
    zcs = [(zc + d) % 4 for d in range(4)]

    def slice_of(slot, i, h=None):
        if h is None:
            return wo.at[slot, x, rows_of(i * 64, 64)]
        return wo.at[slot, x, rows_of(i * 64 + h * 32, 32)]

    out_y = Ring4(
        OY, along_y(ys[1]), along_y(ys[3]), slice_of(0, zc), slice_of(2, zc), slice_of(1, zc),
        (slice_of(2, zc, 0), slice_of(1, zc, 1), slice_of(2, zc), slice_of(1, zc)),
        (slice_of(3, zc, 0), slice_of(3, zc, 1)), (slice_of(3, zc, 0), slice_of(3, zc, 1)),
        wo.at[0, 0, pl.ds(0, 192)],
    )

    near, far = pl.ds(1, 2), 3
    out_z = []
    out_x = []
    for k, slot in enumerate((near, far)):
        piece = functools.partial(slice_of, slot)
        out_z.append(ring_at(OZ + 4 * k, zcs, (along_z(zr), along_z(zl)), piece, piece, wo.at[slot, 0, pl.ds(0, 192)]))
        out_x.append(
            ring_at(
                OX + 4 * k, xs, (along_x(xs[1]), along_x(xs[3])),
                lambda i, s=slot: wo.at[s, i],
                lambda i, h, s=slot: wo.at[s, i, pl.ds(h * 128, 128)],
                wo.at[slot, pl.ds(0, 3)],
            )
        )

    def local(i, src, dst):
        copy = pltpu.make_async_copy(src, dst, lsem.at[i])
        copy.start()
        return copy

    col = pl.ds(pl.multiple_of(x * 128, 128), 128)
    col2 = pl.ds(pl.multiple_of((x // 2) * 128, 128), 128)
    own_rows = pl.ds(pl.multiple_of(y * 512, 512), 512)
    lo, hi = pl.ds(0, 128), pl.ds(128, 128)
    load_tok = local(0, tok_in.at[0], tok.at[x, c])
    load_g = [
        [local(1, w_dk.at[:, col], wg0.at[own_rows, lo]), local(2, w_dv.at[:, col], wg0.at[own_rows, hi])],
        [local(3, w_rk.at[:, col2], wg1.at[own_rows, lo]), local(4, w_rv.at[:, col], wg1.at[own_rows, hi])],
        [local(5, w_dq.at[:, col], wg2.at[own_rows])],
        [local(6, w_rq.at[:, col2], wg3.at[own_rows, lo]), local(7, w_rg.at[:, col], wg3.at[own_rows, hi])],
    ]
    load_o = []
    for i in range(NX):
        src = (w_ro, w_do)[i // 2]
        load_o.append(local(8 + i, src.at[pl.ds((i % 2) * 256, 256)], wo.at[0, i]))

    load_small = [
        local(12 + i, src, dst)
        for i, (src, dst) in enumerate((
            (dec_hbm, dec_in), (lam_hbm, lam_in), (qgain_hbm, qgain_in), (kgain_hbm, kgain_in),
            (rgain_hbm, rgain_in), (dgain_hbm, dgain_in), (ngain_hbm, gain_in), (tab_hbm, tab),
        ))
    ]

    phase("barrier")
    barrier = pltpu.get_barrier_semaphore()
    peers = [along_x(xs[1]), along_x(xs[2]), along_x(xs[3]), along_y(ys[1]), along_y(ys[3]),
             along_z(zr), along_z(zl), partner]
    for peer in peers:
        pl.semaphore_signal(barrier, inc=1, device_id=peer, device_id_type=MESH)
    pl.semaphore_wait(barrier, len(peers))

    phase("loads")
    for copy in load_small:
        copy.wait()
    for d in (1, 2, 3):
        send(DEC + d - 1, dec_in, dec.at[x], along_x(xs[d]))
    dec[x] = dec_in[...]
    for copy in load_o:
        copy.wait()
    out_y.own()
    load_tok.wait()
    tokens_own()
    send(PART, tok.at[x, c], tok.at[x, c], partner)
    for copy in load_g[0]:
        copy.wait()
    weights_own()
    for group in load_g[1:]:
        for copy in group:
            copy.wait()

    lane = lax.broadcasted_iota(jnp.int32, (128, 128), 1)
    sub = lax.broadcasted_iota(jnp.int32, (128, 128), 0)

    phase("tables")
    lane64 = lax.broadcasted_iota(jnp.int32, (64, 128), 1)
    zrow = pl.ds(pl.multiple_of(z * 8, 8), 8)
    for k, ref in enumerate((cosd, sind, cosr, sinr)):
        by_row = tab[k, zrow, :]
        by_col = tab[k]
        is_row = (lane64 % 64) < 32 if k < 2 else lane64 < 64
        for b in range(8):
            ref[b * 64 : b * 64 + 64, :] = jnp.where(is_row, by_row[b : b + 1, :], by_col)

    def rope(u, cos, sin, group):
        half = group // 2
        up = pltpu.roll(u, 128 - half, 1)
        down = pltpu.roll(u, half, 1)
        return u * cos + jnp.where((lane % group) < half, up, down) * sin

    def map_norm(u, gain):
        square = u * u
        first = jnp.sum(jnp.where(lane < 64, square, 0.0), axis=-1, keepdims=True)
        second = jnp.sum(jnp.where(lane < 64, 0.0, square), axis=-1, keepdims=True)
        scale = jnp.where(
            lane < 64, lax.rsqrt(first / 64 + EPS), lax.rsqrt(second / 64 + EPS)
        )
        return u * scale * gain

    order = [xs[0], xs[3], xs[1], xs[2]]

    def block_rows(j):
        return rows_of(order[j] * 128, 128)

    def normalize(j):
        i = order[j]
        for k in range(8):
            r = slice(k * 16, k * 16 + 16)
            w = slice(j * 128 + k * 16, j * 128 + k * 16 + 16)
            a = tok[i, 0, r, :].astype(F32)
            b = tok[i, 1, r, :].astype(F32)
            total = jnp.sum(a * a, axis=-1, keepdims=True) + jnp.sum(b * b, axis=-1, keepdims=True)
            scale = lax.rsqrt(total / D + EPS)
            xn[w, 0:1024] = (a * scale * gain_in[:, 0:1024]).astype(BF16)
            xn[w, 1024:2048] = (b * scale * gain_in[:, 1024:2048]).astype(BF16)

    def project(g, start=0, size=BLOCK):
        ref = wgs[g]
        width = WIDTHS[g]
        step = 256 if size % 256 == 0 else 128
        for j in range(start, start + size, step):
            proj[j : j + step, 0:width] = jnp.dot(
                xn[j : j + step, :], ref[...], preferred_element_type=F32
            )

    def part_send(n, block, start, size):
        ref = tok.at[block, c, pl.ds(start, size)]
        send(PART + n, ref, ref, partner)

    def part_arrived(n, block, start, size):
        arrived(PART + n, tok.at[block, other, pl.ds(start, size)])

    kgain = jnp.concatenate([kgain_in[x][0:1, :], kgain_in[x][1:2, :]], axis=1)

    def keys_values(j):
        r = slice(j * 128, j * 128 + 128)
        a = block_rows(j)
        u = map_norm(proj[r, 0:128], kgain)
        kb[z, r, :] = rope(u, cosd[a, :], sind[a, :], 32).astype(BF16)
        vb[z, :, r] = proj[r, 128:256].T.astype(BF16)

    phase("oy")
    out_y.near()
    out_z[0].own()
    phase("levels")
    for d in (1, 2, 3):
        arrived(DEC + d - 1, dec.at[xs[4 - d]])
    lane8 = lax.broadcasted_iota(jnp.int32, (2, 128), 1)
    offset = jnp.zeros((1, 1), F32)
    head = x // 2
    for b in range(NX):
        level = dec[b]
        for k in (1, 2, 4, 8, 16, 32, 64):
            level = level + jnp.where(lane8 >= k, pltpu.roll(level, k, 1), 0.0)
        row = jnp.where(head == 0, level[0:1, :], level[1:2, :]) + offset
        offset = row[:, 127:128]
        grow[:, b * 128 : b * 128 + 128] = row
        gcol[b * 128 : b * 128 + 128, :] = jnp.broadcast_to(row, (128, 128)).T
    dz[z] = jnp.broadcast_to(offset, (8, 128))

    def kv_step(step, piece):
        for way in (0, 1):
            kv_arrived(step, way, piece)
            if step < 2 or (step == 2 and piece == way):
                kv_send(step + 1, way, piece)

    phase("tok_a")
    tokens_first()
    part_send(1, order[1], 0, 64)
    part_send(2, order[2], 64, 64)
    phase("w0a")
    weights_first()
    ring1.own()
    ring2.own()
    phase("tok_b")
    tokens_second()
    part_send(3, order[1], 64, 64)
    part_send(4, order[2], 0, 64)
    phase("norm0")
    arrived(PART, tok.at[x, other])
    normalize(0)
    phase("oz_near")
    out_z[0].near()
    phase("tok_far_a")
    arrived(TOK + 4, token_half(xs[2], 0))
    part_send(5, order[3], 0, 64)
    phase("norm12")
    for j in (1, 2):
        part_arrived(j, order[j], (j - 1) * 64, 64)
        part_arrived(2 + j, order[j], (2 - j) * 64, 64)
        normalize(j)
    phase("oy_far")
    out_y.far()
    out_z[1].own()
    phase("tok_far_b")
    arrived(TOK + 5, token_half(xs[2], 1))
    part_send(6, order[3], 64, 64)
    phase("norm3")
    part_arrived(5, order[3], 0, 64)
    part_arrived(6, order[3], 64, 64)
    normalize(3)
    phase("w0_far")
    weights_rest()
    phase("project0")
    project(0)
    phase("kv_post")
    for j in range(4):
        keys_values(j)

    zs = [(z + NZ + d) % NZ for d in range(-4, 5)]

    def at_z(d):
        return zs[d + 4]

    kv_rings = [kb.at[pl.ds(0, 7)], vb.at[pl.ds(0, 7)]]

    def kv_send(step, way, piece):
        origin = at_z(-step if way == 0 else step)
        ref = (kb, vb)[piece].at[origin]
        send(KV + 4 * step + 2 * way + piece, ref, ref, along_z(zr if way == 0 else zl), kv_rings[piece])

    def kv_arrived(step, way, piece):
        origin = at_z(-(step + 1) if way == 0 else step + 1)
        arrived(KV + 4 * step + 2 * way + piece, (kb, vb)[piece].at[origin])

    for piece in (0, 1):
        for way in (0, 1):
            kv_send(0, way, piece)

    phase("oz_near_far")
    out_z[0].far()
    out_x[0].own()
    phase("oz_far_near")
    out_z[1].near()
    phase("w1")
    ring1.near()
    phase("k0")
    kv_step(0, 0)
    phase("w2")
    ring2.near()
    ring3.own()
    phase("v0")
    kv_step(0, 1)
    phase("w1_far")
    ring1.far()
    phase("project1")
    project(1)
    phase("states")
    for i in range(NX):
        r = slice(i * 128, i * 128 + 128)
        a = block_rows(i)
        u = rope(proj[r, 0:128], cosr[a, :], sinr[a, :], 64) * (128 ** -0.5)
        rk[a, :] = u.astype(BF16)
        rv[a, :] = proj[r, 128:256].astype(BF16)
    end = dz[z][0:1, :]
    forward_state = jnp.zeros((128, 128), F32)
    backward_state = jnp.zeros((128, 128), F32)
    for i in range(NX):
        r = slice(i * 128, i * 128 + 128)
        key = rk[r, :].astype(F32)
        value = rv[r, :]
        level = gcol[r, :]
        a = (key * jnp.exp(end - level)).T.astype(BF16)
        b = (key * jnp.exp(level)).T.astype(BF16)
        forward_state += jnp.dot(a, value, preferred_element_type=F32)
        backward_state += jnp.dot(b, value, preferred_element_type=F32)
    st[z, 0] = forward_state.astype(BF16)
    st[z, 1] = backward_state.astype(BF16)

    def st_send(step, way):
        origin = at_z(-step if way == 0 else step)
        device = along_z(zr if way == 0 else zl)
        base = ST + 4 * step + 2 * way
        states = st.at[origin] if step < 3 else st.at[origin, way]
        send(base, states, states, device)
        if step < 3 or way == 1:
            send(base + 1, dz.at[origin], dz.at[origin], device)

    def st_step(step):
        for way in (0, 1):
            origin = at_z(-(step + 1) if way == 0 else step + 1)
            base = ST + 4 * step + 2 * way
            arrived(base, st.at[origin] if step < 3 else st.at[origin, way])
            if step < 3 or way == 1:
                arrived(base + 1, dz.at[origin])
            if step < 3:
                st_send(step + 1, way)

    st_send(0, 0)
    st_send(0, 1)

    m_run[...] = jnp.full((4, 1, 256), -jnp.inf, F32)
    l_run[...] = jnp.zeros((4, 1, 256), F32)
    acc[...] = jnp.zeros((4, 128, 256), F32)

    def attend(origins, tiles):
        for q in tiles:
            s = [jnp.dot(kb[o], qbd[q], preferred_element_type=F32) for o in origins]
            before = m_run[q]
            now = before
            for part_s in s:
                now = jnp.maximum(now, jnp.max(part_s, axis=0, keepdims=True))
            shrink = jnp.exp(before - now)
            m_run[q] = now
            total = l_run[q] * shrink
            value = acc[q] * shrink
            for o, part_s in zip(origins, s):
                e = jnp.exp(part_s - now)
                total = total + jnp.sum(e, axis=0, keepdims=True)
                value = value + jnp.dot(vb[o], e.astype(BF16), preferred_element_type=F32)
            l_run[q] = total
            acc[q] = value

    phase("w2_far")
    ring2.far()
    phase("k1")
    kv_step(1, 0)
    phase("project2")
    project(2)
    phase("q_post")
    query_order = [3, 1, 2, 0]
    qgain = jnp.concatenate([qgain_in[x][0:1, :], qgain_in[x][1:2, :]], axis=1)
    for p, i in enumerate(query_order):
        r = slice(i * 128, i * 128 + 128)
        a = block_rows(i)
        u = map_norm(proj[r, 0:128], qgain)
        u = rope(u, cosd[a, :], sind[a, :], 32).astype(BF16).astype(F32) * 0.125
        u = u.T
        s = slice((p % 2) * 128, (p % 2) * 128 + 128)
        qbd[p // 2, :, s] = jnp.where(sub < 64, u, 0.0).astype(BF16)
        qbd[2 + p // 2, :, s] = jnp.where(sub < 64, 0.0, u).astype(BF16)

    phase("v1")
    kv_step(1, 1)
    phase("attend0a")
    attend((z,), (0, 1))
    phase("oz_far_far")
    out_z[1].far()
    out_x[1].own()
    phase("st_step0")
    st_step(0)
    phase("attend0b")
    attend((z,), (2, 3))
    phase("ox_near")
    out_x[0].near()
    phase("attend1a")
    attend((at_z(-1), at_z(1)), (0, 1))
    phase("k2")
    kv_step(2, 0)
    phase("attend1b")
    attend((at_z(-1), at_z(1)), (2, 3))
    phase("w3")
    ring3.near()
    phase("attend2a")
    attend((at_z(-2), at_z(2)), (0, 1))
    phase("v2")
    kv_step(2, 1)
    phase("attend2b")
    attend((at_z(-2), at_z(2)), (2, 3))
    phase("st_step1")
    st_step(1)
    phase("ox_far")
    out_x[1].near()
    phase("w3_far")
    ring3.far()
    phase("project3")
    project(3)
    for i in range(NX):
        r = slice(i * 128, i * 128 + 128)
        a = block_rows(i)
        rq[a, :] = rope(proj[r, 0:128], cosr[a, :], sinr[a, :], 64).astype(BF16)
        gate[i] = proj[r, 128:256].astype(BF16)
    for d, j in ((1, 2), (2, 3), (3, 1)):
        send(GT + d - 1, gate.at[j], gt.at[x], along_x(xs[d]))
    gt[x] = gate[0]

    phase("intra")
    for i in range(NX):
        r = slice(i * 128, i * 128 + 128)
        s = lax.dot_general(rq[r, :], rk[...], (((1,), (1,)), ((), ())), preferred_element_type=F32)
        level = jnp.concatenate([gcol[r, :]] * 4, axis=1)
        w = (s * jnp.exp(-jnp.abs(level - grow[...]))).astype(BF16)
        mix[i] = jnp.dot(w, rv[...], preferred_element_type=F32)

    phase("attend3a")
    attend((at_z(-3), at_z(3)), (0, 2))
    phase("st_step2")
    st_step(2)
    phase("attend3b")
    attend((at_z(-3), at_z(3)), (1, 3))
    phase("kv_last")
    kv_arrived(3, 0, 0)
    kv_arrived(3, 1, 1)

    lane4 = lax.broadcasted_iota(jnp.int32, (1, 4), 1)
    lam = jnp.sum(jnp.where(lane4 == x, lam_in[...], 0.0), axis=-1, keepdims=True)
    dgain = dgain_in[pl.ds(x, 1), :]

    def differ_out(t):
        first = acc[t] / l_run[t]
        second = acc[2 + t] / l_run[2 + t]
        both = first - lam * second
        both = both * lax.rsqrt(jnp.mean(both * both, axis=0, keepdims=True) + EPS)
        for h in range(2):
            j = query_order[2 * t + h]
            feat[j] = (both[:, h * 128 : h * 128 + 128].T * dgain).astype(BF16)

    phase("attend4a")
    attend((at_z(4),), (0, 2))
    phase("differ_out_a")
    differ_out(0)
    send(DF + 1, feat.at[3], df.at[x], along_x(xs[2]))
    send(DF + 2, feat.at[1], df.at[x], along_x(xs[3]))
    phase("st_step3")
    st_step(3)
    phase("carried")
    forward_state = jnp.zeros((128, 128), F32)
    total = jnp.zeros((1, 128), F32)
    for k in range(NZ - 1, -1, -1):
        take = jnp.where(k < z, 1.0, 0.0)
        forward_state += (jnp.exp(total) * take) * st[k, 0].astype(F32)
        total += dz[k][0:1, :] * take
    backward_state = jnp.zeros((128, 128), F32)
    total = jnp.zeros((1, 128), F32)
    for k in range(NZ):
        take = jnp.where(k > z, 1.0, 0.0)
        backward_state += (jnp.exp(total) * take) * st[k, 1].astype(F32)
        total += dz[k][0:1, :] * take
    states = jnp.concatenate([forward_state, backward_state], axis=0).astype(BF16)
    for i in range(NX):
        r = slice(i * 128, i * 128 + 128)
        query = rq[r, :].astype(F32)
        level = gcol[r, :]
        q2 = jnp.concatenate(
            [(query * jnp.exp(level)).astype(BF16), (query * jnp.exp(end - level)).astype(BF16)],
            axis=1,
        )
        total = mix[i] + jnp.dot(q2, states, preferred_element_type=F32)
        mixed[i] = total.astype(BF16)
    send(RM + 1, mixed.at[xs[2]], rm.at[x], along_x(xs[2]))
    send(RM, mixed.at[xs[1]], rm.at[x], along_x(xs[1]))
    send(RM + 2, mixed.at[xs[3]], rm.at[x], along_x(xs[3]))
    rm[x] = mixed[x]
    phase("attend4b")
    attend((at_z(4),), (1, 3))
    phase("differ_out_b")
    differ_out(1)
    send(DF, feat.at[2], df.at[x], along_x(xs[1]))
    df[x] = feat[0]

    phase("ox_far_far")
    for ring in out_x:
        ring.far()
    phase("home_wait_r")
    for d in (1, 2, 3):
        arrived(GT + d - 1, gt.at[xs[4 - d]])
        arrived(RM + d - 1, rm.at[xs[4 - d]])
    phase("home_r")
    for h in range(2):
        a, b = rm[2 * h].astype(F32), rm[2 * h + 1].astype(F32)
        total = jnp.sum(a * a, axis=-1, keepdims=True) + jnp.sum(b * b, axis=-1, keepdims=True)
        scale = lax.rsqrt(total / 256 + EPS)
        for k, m in ((2 * h, a), (2 * h + 1, b)):
            g = gt[k].astype(F32)
            value = (g * jax.nn.sigmoid(g)) * (m * scale * rgain_in[k : k + 1, :])
            fall[:, k * 128 : k * 128 + 128] = value.astype(BF16)
    for k in range(NY):
        w = wo[k].reshape(1024, 512)[0:512]
        total_out[k] = jnp.dot(fall[:, 0:512], w, preferred_element_type=F32)
    phase("home_wait_d")
    for d in (1, 2, 3):
        arrived(DF + d - 1, df.at[xs[4 - d]])
    for k in range(NX):
        fall[:, 512 + k * 128 : 640 + k * 128] = df[k]
    phase("out_dot")
    mine = pl.ds(pl.multiple_of(c * 64, 64), 64)
    theirs = pl.ds(pl.multiple_of(other * 64, 64), 64)
    own_copies = []
    for k in range(NY):
        w = wo[k].reshape(1024, 512)[512:1024]
        total = total_out[k] + jnp.dot(fall[:, 512:1024], w, preferred_element_type=F32)
        part[k] = total.astype(BF16)
        columns = rows_of(ys[(0, 1, 3, 2)[k]] * 512, 512)
        send(OUT + k, part.at[k, theirs], out.at[1, :, columns], partner)
        own_copies.append(local(8 + k, part.at[k, mine], out.at[0, :, columns]))
    phase("out_wait")
    for k in range(NY):
        arrived(OUT + k, out.at[1, :, rows_of(ys[(0, 1, 3, 2)[k]] * 512, 512)])
    for copy in own_copies:
        copy.wait()
    phase("drain")
    for copy in sent:
        if copy is not None:
            copy.wait_send()
    for n, ref in rings_sent.values():
        pltpu.make_async_remote_copy(
            src_ref=ref, dst_ref=ref, send_sem=ssem.at[n], recv_sem=rsem.at[0],
            device_id=partner, device_id_type=MESH,
        ).wait_send()
    assert len(sent) == SENDS, len(sent)
    phase(None)


def body(
    tokens, norm_gain, retain_query, retain_key, retain_value, retain_gate, differ_query,
    differ_key, differ_value, log_decay, lambdas, query_gain, key_gain, retain_gain,
    differ_gain, retain_out, differ_out,
):
    hbm = pl.BlockSpec(memory_space=pltpu.HBM)
    V = pltpu.VMEM
    parts = pl.pallas_call(
        kernel,
        out_shape=jax.ShapeDtypeStruct((2, 64, D), BF16),
        in_specs=[hbm] * 18,
        out_specs=hbm,
        scratch_shapes=[
            V((2, 128), F32), V((1, 4), F32), V((4, 2, 64), F32), V((4, 2, 64), F32),
            V((4, 128), F32), V((4, 128), F32), V((1, D), F32), V((4, 64, 128), F32),
            V((NX, 2, 128, 1024), BF16),
            V((BLOCK, D), BF16),
            V((D, 256), BF16), V((D, 256), BF16), V((D, 128), BF16), V((D, 256), BF16),
            V((NY, NX, 256, 512), BF16),
            V((NX, 2, 128), F32),
            V((NZ, BLOCK, 128), BF16),
            V((NZ, 128, BLOCK), BF16),
            V((NZ, 2, 128, 128), BF16),
            V((NZ, 8, 128), F32),
            V((BLOCK, 128), F32), V((BLOCK, 128), F32), V((BLOCK, 128), F32), V((BLOCK, 128), F32),
            V((BLOCK, 256), F32), V((BLOCK, 128), F32),
            V((4, 128, 256), BF16),
            V((4, 1, 256), F32), V((4, 1, 256), F32), V((4, 128, 256), F32),
            V((BLOCK, 128), BF16), V((BLOCK, 128), BF16), V((BLOCK, 128), BF16),
            V((1, BLOCK), F32), V((BLOCK, 128), F32),
            V((NX, 128, 128), F32),
            V((NX, 128, 128), BF16), V((NX, 128, 128), BF16),
            V((NX, 128, 128), BF16), V((NX, 128, 128), BF16), V((NX, 128, 128), BF16),
            V((128, 1024), BF16),
            V((NY, 128, 512), BF16),
            V((NX, 128, 128), BF16), V((NY, 128, 512), F32),
            pltpu.SemaphoreType.DMA((SENDS,)),
            pltpu.SemaphoreType.DMA((COPIES,)),
            pltpu.SemaphoreType.DMA((LOCALS,)),
        ],
        compiler_params=pltpu.CompilerParams(
            collective_id=0, has_side_effects=True, vmem_limit_bytes=67000000
        ),
    )(
        tokens, retain_query, retain_key, retain_value, retain_gate, differ_query, differ_key,
        differ_value, retain_out, differ_out, log_decay[0].T, lambdas.reshape(1, 4), query_gain,
        key_gain, retain_gain.reshape(4, 128), differ_gain.reshape(4, 128), norm_gain.reshape(1, D),
        jnp.asarray(rope_tables()),
    )
    return (parts[0:1].astype(F32) + parts[1:2].astype(F32)).astype(BF16)


def solution(mesh):
    in_specs = (
        P("fs", "sp", "tp"), P(),
        P("fs", "tp"), P("fs", "tp"), P("fs", "tp"), P("fs", "tp"), P("fs", "tp"), P("fs", "tp"), P("fs", "tp"),
        P("fs", "sp", "tp"),
        P("tp"), P("tp", None, None), P("tp", None, None), P("tp"), P("tp"),
        P("tp", "fs"), P("tp", "fs"),
    )
    out_specs = P("fs", ("sp", "tp"), None)
    return jax.shard_map(body, mesh=mesh, in_specs=in_specs, out_specs=out_specs, check_vma=False)
```

```python
import functools

import numpy as np
import jax
import jax.numpy as jnp
from jax import lax
from jax.experimental import pallas as pl
from jax.experimental.pallas import tpu as pltpu
from jax.sharding import PartitionSpec as P

F32 = jnp.float32
BF16 = jnp.bfloat16
MESH = pl.DeviceIdType.MESH
EPS = 1e-06
ROPE_BASE = 10000.0
NX, NY, NZ = 4, 4, 8
ROWS = 128
BLOCK = NX * ROWS
D = 2048
WIDTHS = (256, 256, 128, 256)

TOK = 0
PART = 8
W0 = 16
W1 = 24
W2 = 28
W3 = 32
OY = 36
OZ = 40
OX = 48
DEC = 56
KV = 59
ST = 75
DF = 91
GT = 94
RM = 97
OUT = 100
COPIES = 104
SENDS = 50
LOCALS = 20


def rope_tables():
    lane = np.arange(128)
    value = np.arange(64, dtype=np.float64)[:, None]
    tables = []
    for group in (32, 64):
        inverse = ROPE_BASE ** (-2.0 * ((lane % group) % (group // 2)) / group)
        angle = value * inverse[None, :]
        sign = np.where((lane % group) < group // 2, -1.0, 1.0)[None, :]
        tables += [np.cos(angle), np.sin(angle) * sign]
    return np.stack(tables).astype(np.float32)


class Phases:
    def __init__(self):
        self.scope = None

    def __call__(self, name):
        if self.scope is not None:
            self.scope.__exit__(None, None, None)
        self.scope = jax.named_scope(name) if name else None
        if self.scope is not None:
            self.scope.__enter__()


def kernel(
    tok_in, w_rq, w_rk, w_rv, w_rg, w_dq, w_dk, w_dv, w_ro, w_do,
    dec_hbm, lam_hbm, qgain_hbm, kgain_hbm, rgain_hbm, dgain_hbm, ngain_hbm, tab_hbm,
    out,
    dec_in, lam_in, qgain_in, kgain_in, rgain_in, dgain_in, gain_in, tab, tok, xn, wg0, wg1, wg2, wg3, wo, dec, kb, vb, st, dz, cosd, sind, cosr, sinr, proj, proj2, qbd,
    m_run, l_run, acc, rq, rk, rv, grow, gcol, mix, gate, feat, df, gt, rm, fall, part, mixed, total_out,
    ssem, rsem, lsem,
):
    phase = Phases()
    sp = lax.axis_index("sp")
    z, x = sp // NX, sp % NX
    y = lax.axis_index("fs")
    c = lax.axis_index("tp")
    other = 1 - c

    def along_x(i):
        return {"sp": z * NX + i}

    def along_y(i):
        return {"fs": i}

    def along_z(i):
        return {"sp": i * NX + x}

    partner = {"tp": other}
    xs = [x, (x + 1) % NX, (x + 2) % NX, (x + 3) % NX]
    ys = [y, (y + 1) % NY, (y + 2) % NY, (y + 3) % NY]
    zr, zl = (z + 1) % NZ, (z + NZ - 1) % NZ

    sent = []
    rings_sent = {}

    def send(i, src, dst, device, ring=None):
        n = len(sent) if ring is None else rings_sent.setdefault(id(ring), (len(sent), ring))[0]
        copy = pltpu.make_async_remote_copy(
            src_ref=src, dst_ref=dst, send_sem=ssem.at[n], recv_sem=rsem.at[i],
            device_id=device, device_id_type=MESH,
        )
        copy.start()
        if n == len(sent):
            sent.append(copy if ring is None else None)

    def arrived(i, ref):
        pltpu.make_async_remote_copy(
            src_ref=ref, dst_ref=ref, send_sem=ssem.at[0], recv_sem=rsem.at[i],
            device_id=partner, device_id_type=MESH,
        ).wait_recv()

    class Ring4:
        def __init__(self, base, right, left, own, to_right, to_left, half, onward, far, three):
            self.base, self.right, self.left = base, right, left
            self.src, self.to_right, self.to_left, self.half = own, to_right, to_left, half
            self.onward, self.far_half = onward, far
            self.three = three

        def own(self):
            send(self.base, self.src, self.to_right, self.right, self.three)
            send(self.base + 1, self.src, self.to_left, self.left, self.three)

        def wait(self):
            arrived(self.base, self.half[2])
            arrived(self.base + 1, self.half[3])

        def forward(self):
            send(self.base + 2, self.half[0], self.onward[0], self.right, self.three)
            send(self.base + 3, self.half[1], self.onward[1], self.left, self.three)

        def near(self):
            self.wait()
            self.forward()

        def far(self):
            arrived(self.base + 2, self.far_half[0])
            arrived(self.base + 3, self.far_half[1])

    def ring_at(base, at, sides, full, half, three):
        return Ring4(
            base, sides[0], sides[1], full(at[0]), full(at[0]), full(at[0]),
            (half(at[3], 0), half(at[1], 1), full(at[3]), full(at[1])),
            (half(at[3], 0), half(at[1], 1)), (half(at[2], 0), half(at[2], 1)), three,
        )

    wgs = (wg0, wg1, wg2, wg3)
    def rows_of(start, size):
        return pl.ds(pl.multiple_of(start, size & -size), size)

    def token_half(i, h):
        return tok.at[i, c, pl.ds(h * 64, 64)]

    six = tok.at[pl.ds(0, 3), 0]

    def token_send(n, i, h, to):
        send(TOK + n, token_half(i, h), token_half(i, h), along_x(xs[to]), six)

    def tokens_own():
        for n, h, to in ((0, 0, 1), (1, 1, 3), (2, 1, 1), (3, 0, 3)):
            token_send(n, xs[0], h, to)

    def tokens_first():
        arrived(TOK, token_half(xs[3], 0))
        token_send(4, xs[3], 0, 1)
        arrived(TOK + 1, token_half(xs[1], 1))
        token_send(5, xs[1], 1, 3)

    def tokens_second():
        arrived(TOK + 2, token_half(xs[3], 1))
        arrived(TOK + 3, token_half(xs[1], 0))

    def weight_ring(base, ref, start, size):
        return ring_at(
            base, ys, (along_y(ys[1]), along_y(ys[3])),
            lambda i: ref.at[rows_of(i * 512 + start, size)],
            lambda i, h: ref.at[rows_of(i * 512 + start + h * (size // 2), size // 2)],
            ref.at[pl.ds(start, 3 * size)],
        )

    def weight_half(i, h):
        return wg0.at[rows_of(i * 512 + h * 256, 256)]

    three_blocks = wg0.at[pl.ds(0, 1536)]

    def weight_send(n, i, h, to):
        send(W0 + n, weight_half(i, h), weight_half(i, h), along_y(ys[to]), three_blocks)

    def weights_own():
        for n, h, to in ((0, 0, 1), (1, 1, 3), (2, 1, 1), (3, 0, 3)):
            weight_send(n, ys[0], h, to)

    def weights_first():
        arrived(W0, weight_half(ys[3], 0))
        weight_send(4, ys[3], 0, 1)
        arrived(W0 + 1, weight_half(ys[1], 1))
        weight_send(5, ys[1], 1, 3)

    def weights_rest():
        arrived(W0 + 2, weight_half(ys[3], 1))
        arrived(W0 + 3, weight_half(ys[1], 0))
        arrived(W0 + 4, weight_half(ys[2], 0))
        arrived(W0 + 5, weight_half(ys[2], 1))

    ring1 = weight_ring(W1, wg1, 0, 512)
    ring2 = weight_ring(W2, wg2, 0, 512)
    ring3 = weight_ring(W3, wg3, 0, 512)

    zc = z % 4
    zcs = [(zc + d) % 4 for d in range(4)]

    def slice_of(slot, i, h=None):
        if h is None:
            return wo.at[slot, x, rows_of(i * 64, 64)]
        return wo.at[slot, x, rows_of(i * 64 + h * 32, 32)]

    out_y = Ring4(
        OY, along_y(ys[1]), along_y(ys[3]), slice_of(0, zc), slice_of(2, zc), slice_of(1, zc),
        (slice_of(2, zc, 0), slice_of(1, zc, 1), slice_of(2, zc), slice_of(1, zc)),
        (slice_of(3, zc, 0), slice_of(3, zc, 1)), (slice_of(3, zc, 0), slice_of(3, zc, 1)),
        wo.at[0, 0, pl.ds(0, 192)],
    )

    near, far = pl.ds(1, 2), 3
    out_z = []
    out_x = []
    for k, slot in enumerate((near, far)):
        piece = functools.partial(slice_of, slot)
        out_z.append(ring_at(OZ + 4 * k, zcs, (along_z(zr), along_z(zl)), piece, piece, wo.at[slot, 0, pl.ds(0, 192)]))
        out_x.append(
            ring_at(
                OX + 4 * k, xs, (along_x(xs[1]), along_x(xs[3])),
                lambda i, s=slot: wo.at[s, i],
                lambda i, h, s=slot: wo.at[s, i, pl.ds(h * 128, 128)],
                wo.at[slot, pl.ds(0, 3)],
            )
        )

    def local(i, src, dst):
        copy = pltpu.make_async_copy(src, dst, lsem.at[i])
        copy.start()
        return copy

    col = pl.ds(pl.multiple_of(x * 128, 128), 128)
    col2 = pl.ds(pl.multiple_of((x // 2) * 128, 128), 128)
    own_rows = pl.ds(pl.multiple_of(y * 512, 512), 512)
    lo, hi = pl.ds(0, 128), pl.ds(128, 128)
    load_tok = local(0, tok_in.at[0], tok.at[x, c])
    load_g = [
        [local(1, w_dk.at[:, col], wg0.at[own_rows, lo]), local(2, w_dv.at[:, col], wg0.at[own_rows, hi])],
        [local(3, w_rk.at[:, col2], wg1.at[own_rows, lo]), local(4, w_rv.at[:, col], wg1.at[own_rows, hi])],
        [local(5, w_dq.at[:, col], wg2.at[own_rows])],
        [local(6, w_rq.at[:, col2], wg3.at[own_rows, lo]), local(7, w_rg.at[:, col], wg3.at[own_rows, hi])],
    ]
    load_o = []
    for i in range(NX):
        src = (w_ro, w_do)[i // 2]
        load_o.append(local(8 + i, src.at[pl.ds((i % 2) * 256, 256)], wo.at[0, i]))

    load_small = [
        local(12 + i, src, dst)
        for i, (src, dst) in enumerate((
            (dec_hbm, dec_in), (lam_hbm, lam_in), (qgain_hbm, qgain_in), (kgain_hbm, kgain_in),
            (rgain_hbm, rgain_in), (dgain_hbm, dgain_in), (ngain_hbm, gain_in), (tab_hbm, tab),
        ))
    ]

    phase("barrier")
    barrier = pltpu.get_barrier_semaphore()
    peers = [along_x(xs[1]), along_x(xs[2]), along_x(xs[3]), along_y(ys[1]), along_y(ys[3]),
             along_z(zr), along_z(zl), partner]
    for peer in peers:
        pl.semaphore_signal(barrier, inc=1, device_id=peer, device_id_type=MESH)
    pl.semaphore_wait(barrier, len(peers))

    phase("loads")
    for copy in load_small:
        copy.wait()
    for d in (1, 2, 3):
        send(DEC + d - 1, dec_in, dec.at[x], along_x(xs[d]))
    dec[x] = dec_in[...]
    for copy in load_o:
        copy.wait()
    out_y.own()
    load_tok.wait()
    tokens_own()
    send(PART, tok.at[x, c], tok.at[x, c], partner)
    for copy in load_g[0]:
        copy.wait()
    weights_own()
    for group in load_g[1:]:
        for copy in group:
            copy.wait()

    lane = lax.broadcasted_iota(jnp.int32, (128, 128), 1)
    sub = lax.broadcasted_iota(jnp.int32, (128, 128), 0)

    phase("tables")
    lane64 = lax.broadcasted_iota(jnp.int32, (64, 128), 1)
    zrow = pl.ds(pl.multiple_of(z * 8, 8), 8)
    for k, ref in enumerate((cosd, sind, cosr, sinr)):
        by_row = tab[k, zrow, :]
        by_col = tab[k]
        is_row = (lane64 % 64) < 32 if k < 2 else lane64 < 64
        for b in range(8):
            ref[b * 64 : b * 64 + 64, :] = jnp.where(is_row, by_row[b : b + 1, :], by_col)

    def rope(u, cos, sin, group):
        half = group // 2
        up = pltpu.roll(u, 128 - half, 1)
        down = pltpu.roll(u, half, 1)
        return u * cos + jnp.where((lane % group) < half, up, down) * sin

    def map_norm(u, gain):
        square = u * u
        first = jnp.sum(jnp.where(lane < 64, square, 0.0), axis=-1, keepdims=True)
        second = jnp.sum(jnp.where(lane < 64, 0.0, square), axis=-1, keepdims=True)
        scale = jnp.where(
            lane < 64, lax.rsqrt(first / 64 + EPS), lax.rsqrt(second / 64 + EPS)
        )
        return u * scale * gain

    order = [xs[0], xs[3], xs[1], xs[2]]

    def block_rows(j):
        return rows_of(order[j] * 128, 128)

    def normalize(j):
        i = order[j]
        for k in range(8):
            r = slice(k * 16, k * 16 + 16)
            w = slice(j * 128 + k * 16, j * 128 + k * 16 + 16)
            a = tok[i, 0, r, :].astype(F32)
            b = tok[i, 1, r, :].astype(F32)
            total = jnp.sum(a * a, axis=-1, keepdims=True) + jnp.sum(b * b, axis=-1, keepdims=True)
            scale = lax.rsqrt(total / D + EPS)
            xn[w, 0:1024] = (a * scale * gain_in[:, 0:1024]).astype(BF16)
            xn[w, 1024:2048] = (b * scale * gain_in[:, 1024:2048]).astype(BF16)

    def project(g, start=0, size=BLOCK):
        ref = wgs[g]
        width = WIDTHS[g]
        step = 256 if size % 256 == 0 else 128
        for j in range(start, start + size, step):
            proj[j : j + step, 0:width] = jnp.dot(
                xn[j : j + step, :], ref[...], preferred_element_type=F32
            )

    def part_send(n, block, start, size):
        ref = tok.at[block, c, pl.ds(start, size)]
        send(PART + n, ref, ref, partner)

    def part_arrived(n, block, start, size):
        arrived(PART + n, tok.at[block, other, pl.ds(start, size)])

    kgain = jnp.concatenate([kgain_in[x][0:1, :], kgain_in[x][1:2, :]], axis=1)

    def keys_values(j):
        r = slice(j * 128, j * 128 + 128)
        a = block_rows(j)
        u = map_norm(proj[r, 0:128], kgain)
        kb[z, r, :] = rope(u, cosd[a, :], sind[a, :], 32).astype(BF16)
        vb[z, :, r] = proj[r, 128:256].T.astype(BF16)

    phase("oy")
    out_y.near()
    out_z[0].own()
    phase("levels")
    for d in (1, 2, 3):
        arrived(DEC + d - 1, dec.at[xs[4 - d]])
    lane8 = lax.broadcasted_iota(jnp.int32, (2, 128), 1)
    offset = jnp.zeros((1, 1), F32)
    head = x // 2
    for b in range(NX):
        level = dec[b]
        for k in (1, 2, 4, 8, 16, 32, 64):
            level = level + jnp.where(lane8 >= k, pltpu.roll(level, k, 1), 0.0)
        row = jnp.where(head == 0, level[0:1, :], level[1:2, :]) + offset
        offset = row[:, 127:128]
        grow[:, b * 128 : b * 128 + 128] = row
        gcol[b * 128 : b * 128 + 128, :] = jnp.broadcast_to(row, (128, 128)).T
    dz[z] = jnp.broadcast_to(offset, (8, 128))

    def kv_step(step, piece):
        for way in (0, 1):
            kv_arrived(step, way, piece)
            if step < 2 or (step == 2 and piece == way):
                kv_send(step + 1, way, piece)

    phase("tok_a")
    tokens_first()
    part_send(1, order[1], 0, 64)
    part_send(2, order[2], 64, 64)
    phase("w0a")
    weights_first()
    ring1.own()
    ring2.own()
    phase("tok_b")
    tokens_second()
    part_send(3, order[1], 64, 64)
    part_send(4, order[2], 0, 64)
    phase("norm0")
    arrived(PART, tok.at[x, other])
    normalize(0)
    phase("oz_near")
    out_z[0].near()
    phase("tok_far_a")
    arrived(TOK + 4, token_half(xs[2], 0))
    part_send(5, order[3], 0, 64)
    phase("norm12")
    for j in (1, 2):
        part_arrived(j, order[j], (j - 1) * 64, 64)
        part_arrived(2 + j, order[j], (2 - j) * 64, 64)
        normalize(j)
    phase("oy_far")
    out_y.far()
    out_z[1].own()
    phase("tok_far_b")
    arrived(TOK + 5, token_half(xs[2], 1))
    part_send(6, order[3], 64, 64)
    phase("norm3")
    part_arrived(5, order[3], 0, 64)
    part_arrived(6, order[3], 64, 64)
    normalize(3)
    phase("w0_far")
    weights_rest()
    phase("project0")
    project(0)
    phase("kv_post")
    for j in range(4):
        keys_values(j)

    zs = [(z + NZ + d) % NZ for d in range(-4, 5)]

    def at_z(d):
        return zs[d + 4]

    kv_rings = [kb.at[pl.ds(0, 7)], vb.at[pl.ds(0, 7)]]

    def kv_send(step, way, piece):
        origin = at_z(-step if way == 0 else step)
        ref = (kb, vb)[piece].at[origin]
        send(KV + 4 * step + 2 * way + piece, ref, ref, along_z(zr if way == 0 else zl), kv_rings[piece])

    def kv_arrived(step, way, piece):
        origin = at_z(-(step + 1) if way == 0 else step + 1)
        arrived(KV + 4 * step + 2 * way + piece, (kb, vb)[piece].at[origin])

    for piece in (0, 1):
        for way in (0, 1):
            kv_send(0, way, piece)

    phase("oz_near_far")
    out_z[0].far()
    out_x[0].own()
    phase("oz_far_near")
    out_z[1].near()
    phase("w1")
    ring1.near()
    phase("k0")
    kv_step(0, 0)
    phase("w2")
    ring2.near()
    ring3.own()
    phase("v0")
    kv_step(0, 1)
    phase("w1_far")
    ring1.far()
    phase("project1")
    project(1)
    phase("states")
    for i in range(NX):
        r = slice(i * 128, i * 128 + 128)
        a = block_rows(i)
        u = rope(proj[r, 0:128], cosr[a, :], sinr[a, :], 64) * (128 ** -0.5)
        rk[a, :] = u.astype(BF16)
        rv[a, :] = proj[r, 128:256].astype(BF16)
    end = dz[z][0:1, :]
    forward_state = jnp.zeros((128, 128), F32)
    backward_state = jnp.zeros((128, 128), F32)
    for i in range(NX):
        r = slice(i * 128, i * 128 + 128)
        key = rk[r, :].astype(F32)
        value = rv[r, :]
        level = gcol[r, :]
        a = (key * jnp.exp(end - level)).T.astype(BF16)
        b = (key * jnp.exp(level)).T.astype(BF16)
        forward_state += jnp.dot(a, value, preferred_element_type=F32)
        backward_state += jnp.dot(b, value, preferred_element_type=F32)
    st[z, 0] = forward_state.astype(BF16)
    st[z, 1] = backward_state.astype(BF16)

    def st_send(step, way):
        origin = at_z(-step if way == 0 else step)
        device = along_z(zr if way == 0 else zl)
        base = ST + 4 * step + 2 * way
        states = st.at[origin] if step < 3 else st.at[origin, way]
        send(base, states, states, device)
        if step < 3 or way == 1:
            send(base + 1, dz.at[origin], dz.at[origin], device)

    def st_step(step):
        for way in (0, 1):
            origin = at_z(-(step + 1) if way == 0 else step + 1)
            base = ST + 4 * step + 2 * way
            arrived(base, st.at[origin] if step < 3 else st.at[origin, way])
            if step < 3 or way == 1:
                arrived(base + 1, dz.at[origin])
            if step < 3:
                st_send(step + 1, way)

    st_send(0, 0)
    st_send(0, 1)

    m_run[...] = jnp.full((4, 1, 256), -jnp.inf, F32)
    l_run[...] = jnp.zeros((4, 1, 256), F32)
    acc[...] = jnp.zeros((4, 128, 256), F32)

    def attend(origins, tiles):
        for q in tiles:
            s = [jnp.dot(kb[o], qbd[q], preferred_element_type=F32) for o in origins]
            before = m_run[q]
            now = before
            for part_s in s:
                now = jnp.maximum(now, jnp.max(part_s, axis=0, keepdims=True))
            shrink = jnp.exp(before - now)
            m_run[q] = now
            total = l_run[q] * shrink
            value = acc[q] * shrink
            for o, part_s in zip(origins, s):
                e = jnp.exp(part_s - now)
                total = total + jnp.sum(e, axis=0, keepdims=True)
                value = value + jnp.dot(vb[o], e.astype(BF16), preferred_element_type=F32)
            l_run[q] = total
            acc[q] = value

    phase("w2_far")
    ring2.far()
    phase("k1")
    kv_step(1, 0)
    phase("project2")
    project(2)
    phase("q_post")
    query_order = [3, 1, 2, 0]
    qgain = jnp.concatenate([qgain_in[x][0:1, :], qgain_in[x][1:2, :]], axis=1)
    for p, i in enumerate(query_order):
        r = slice(i * 128, i * 128 + 128)
        a = block_rows(i)
        u = map_norm(proj[r, 0:128], qgain)
        u = rope(u, cosd[a, :], sind[a, :], 32).astype(BF16).astype(F32) * 0.125
        u = u.T
        s = slice((p % 2) * 128, (p % 2) * 128 + 128)
        qbd[p // 2, :, s] = jnp.where(sub < 64, u, 0.0).astype(BF16)
        qbd[2 + p // 2, :, s] = jnp.where(sub < 64, 0.0, u).astype(BF16)

    phase("attend0a")
    attend((z,), (0, 1))
    phase("v1")
    kv_step(1, 1)
    phase("oz_far_far")
    out_z[1].far()
    out_x[1].own()
    phase("attend0b")
    attend((z,), (2, 3))
    phase("st_step0")
    st_step(0)
    phase("ox_near")
    out_x[0].near()
    phase("attend1a")
    attend((at_z(-1), at_z(1)), (0, 1))
    phase("k2")
    kv_step(2, 0)
    phase("attend1b")
    attend((at_z(-1), at_z(1)), (2, 3))
    phase("w3")
    ring3.near()
    phase("attend2a")
    attend((at_z(-2), at_z(2)), (0, 1))
    phase("v2")
    kv_step(2, 1)
    phase("attend2b")
    attend((at_z(-2), at_z(2)), (2, 3))
    phase("st_step1")
    st_step(1)
    phase("ox_far")
    out_x[1].near()
    phase("attend3a")
    attend((at_z(-3), at_z(3)), (0, 2))
    phase("st_step2")
    st_step(2)
    phase("w3_far")
    ring3.far()
    phase("project3")
    project(3)
    for i in range(NX):
        r = slice(i * 128, i * 128 + 128)
        a = block_rows(i)
        rq[a, :] = rope(proj[r, 0:128], cosr[a, :], sinr[a, :], 64).astype(BF16)
        gate[i] = proj[r, 128:256].astype(BF16)
    for d, j in ((1, 2), (2, 3), (3, 1)):
        send(GT + d - 1, gate.at[j], gt.at[x], along_x(xs[d]))
    gt[x] = gate[0]

    phase("intra")
    for i in range(NX):
        r = slice(i * 128, i * 128 + 128)
        s = lax.dot_general(rq[r, :], rk[...], (((1,), (1,)), ((), ())), preferred_element_type=F32)
        level = jnp.concatenate([gcol[r, :]] * 4, axis=1)
        w = (s * jnp.exp(-jnp.abs(level - grow[...]))).astype(BF16)
        mix[i] = jnp.dot(w, rv[...], preferred_element_type=F32)

    phase("attend3b")
    attend((at_z(-3), at_z(3)), (1, 3))
    phase("kv_last")
    kv_arrived(3, 0, 0)
    kv_arrived(3, 1, 1)

    lane4 = lax.broadcasted_iota(jnp.int32, (1, 4), 1)
    lam = jnp.sum(jnp.where(lane4 == x, lam_in[...], 0.0), axis=-1, keepdims=True)
    dgain = dgain_in[pl.ds(x, 1), :]

    def differ_out(t):
        first = acc[t] / l_run[t]
        second = acc[2 + t] / l_run[2 + t]
        both = first - lam * second
        both = both * lax.rsqrt(jnp.mean(both * both, axis=0, keepdims=True) + EPS)
        for h in range(2):
            j = query_order[2 * t + h]
            feat[j] = (both[:, h * 128 : h * 128 + 128].T * dgain).astype(BF16)

    phase("attend4a")
    attend((at_z(4),), (0, 2))
    phase("differ_out_a")
    differ_out(0)
    send(DF + 1, feat.at[3], df.at[x], along_x(xs[2]))
    send(DF + 2, feat.at[1], df.at[x], along_x(xs[3]))
    phase("st_step3")
    st_step(3)
    phase("carried")
    forward_state = jnp.zeros((128, 128), F32)
    total = jnp.zeros((1, 128), F32)
    for k in range(NZ - 1, -1, -1):
        take = jnp.where(k < z, 1.0, 0.0)
        forward_state += (jnp.exp(total) * take) * st[k, 0].astype(F32)
        total += dz[k][0:1, :] * take
    backward_state = jnp.zeros((128, 128), F32)
    total = jnp.zeros((1, 128), F32)
    for k in range(NZ):
        take = jnp.where(k > z, 1.0, 0.0)
        backward_state += (jnp.exp(total) * take) * st[k, 1].astype(F32)
        total += dz[k][0:1, :] * take
    states = jnp.concatenate([forward_state, backward_state], axis=0).astype(BF16)
    for i in range(NX):
        r = slice(i * 128, i * 128 + 128)
        query = rq[r, :].astype(F32)
        level = gcol[r, :]
        q2 = jnp.concatenate(
            [(query * jnp.exp(level)).astype(BF16), (query * jnp.exp(end - level)).astype(BF16)],
            axis=1,
        )
        total = mix[i] + jnp.dot(q2, states, preferred_element_type=F32)
        mixed[i] = total.astype(BF16)
    send(RM + 1, mixed.at[xs[2]], rm.at[x], along_x(xs[2]))
    send(RM, mixed.at[xs[1]], rm.at[x], along_x(xs[1]))
    send(RM + 2, mixed.at[xs[3]], rm.at[x], along_x(xs[3]))
    rm[x] = mixed[x]
    phase("attend4b")
    attend((at_z(4),), (1, 3))
    phase("differ_out_b")
    differ_out(1)
    send(DF, feat.at[2], df.at[x], along_x(xs[1]))
    df[x] = feat[0]

    phase("ox_far_far")
    for ring in out_x:
        ring.far()
    phase("home_wait_r")
    for d in (1, 2, 3):
        arrived(GT + d - 1, gt.at[xs[4 - d]])
        arrived(RM + d - 1, rm.at[xs[4 - d]])
    phase("home_r")
    for h in range(2):
        a, b = rm[2 * h].astype(F32), rm[2 * h + 1].astype(F32)
        total = jnp.sum(a * a, axis=-1, keepdims=True) + jnp.sum(b * b, axis=-1, keepdims=True)
        scale = lax.rsqrt(total / 256 + EPS)
        for k, m in ((2 * h, a), (2 * h + 1, b)):
            g = gt[k].astype(F32)
            value = (g * jax.nn.sigmoid(g)) * (m * scale * rgain_in[k : k + 1, :])
            fall[:, k * 128 : k * 128 + 128] = value.astype(BF16)
    for k in range(NY):
        w = wo[k].reshape(1024, 512)[0:512]
        total_out[k] = jnp.dot(fall[:, 0:512], w, preferred_element_type=F32)
    phase("home_wait_d")
    for d in (1, 2, 3):
        arrived(DF + d - 1, df.at[xs[4 - d]])
    for k in range(NX):
        fall[:, 512 + k * 128 : 640 + k * 128] = df[k]
    phase("out_dot")
    mine = pl.ds(pl.multiple_of(c * 64, 64), 64)
    theirs = pl.ds(pl.multiple_of(other * 64, 64), 64)
    own_copies = []
    for k in range(NY):
        w = wo[k].reshape(1024, 512)[512:1024]
        total = total_out[k] + jnp.dot(fall[:, 512:1024], w, preferred_element_type=F32)
        part[k] = total.astype(BF16)
        columns = rows_of(ys[(0, 1, 3, 2)[k]] * 512, 512)
        send(OUT + k, part.at[k, theirs], out.at[1, :, columns], partner)
        own_copies.append(local(8 + k, part.at[k, mine], out.at[0, :, columns]))
    phase("out_wait")
    for k in range(NY):
        arrived(OUT + k, out.at[1, :, rows_of(ys[(0, 1, 3, 2)[k]] * 512, 512)])
    for copy in own_copies:
        copy.wait()
    phase("drain")
    for copy in sent:
        if copy is not None:
            copy.wait_send()
    for n, ref in rings_sent.values():
        pltpu.make_async_remote_copy(
            src_ref=ref, dst_ref=ref, send_sem=ssem.at[n], recv_sem=rsem.at[0],
            device_id=partner, device_id_type=MESH,
        ).wait_send()
    assert len(sent) == SENDS, len(sent)
    phase(None)


def body(
    tokens, norm_gain, retain_query, retain_key, retain_value, retain_gate, differ_query,
    differ_key, differ_value, log_decay, lambdas, query_gain, key_gain, retain_gain,
    differ_gain, retain_out, differ_out,
):
    hbm = pl.BlockSpec(memory_space=pltpu.HBM)
    V = pltpu.VMEM
    parts = pl.pallas_call(
        kernel,
        out_shape=jax.ShapeDtypeStruct((2, 64, D), BF16),
        in_specs=[hbm] * 18,
        out_specs=hbm,
        scratch_shapes=[
            V((2, 128), F32), V((1, 4), F32), V((4, 2, 64), F32), V((4, 2, 64), F32),
            V((4, 128), F32), V((4, 128), F32), V((1, D), F32), V((4, 64, 128), F32),
            V((NX, 2, 128, 1024), BF16),
            V((BLOCK, D), BF16),
            V((D, 256), BF16), V((D, 256), BF16), V((D, 128), BF16), V((D, 256), BF16),
            V((NY, NX, 256, 512), BF16),
            V((NX, 2, 128), F32),
            V((NZ, BLOCK, 128), BF16),
            V((NZ, 128, BLOCK), BF16),
            V((NZ, 2, 128, 128), BF16),
            V((NZ, 8, 128), F32),
            V((BLOCK, 128), F32), V((BLOCK, 128), F32), V((BLOCK, 128), F32), V((BLOCK, 128), F32),
            V((BLOCK, 256), F32), V((BLOCK, 128), F32),
            V((4, 128, 256), BF16),
            V((4, 1, 256), F32), V((4, 1, 256), F32), V((4, 128, 256), F32),
            V((BLOCK, 128), BF16), V((BLOCK, 128), BF16), V((BLOCK, 128), BF16),
            V((1, BLOCK), F32), V((BLOCK, 128), F32),
            V((NX, 128, 128), F32),
            V((NX, 128, 128), BF16), V((NX, 128, 128), BF16),
            V((NX, 128, 128), BF16), V((NX, 128, 128), BF16), V((NX, 128, 128), BF16),
            V((128, 1024), BF16),
            V((NY, 128, 512), BF16),
            V((NX, 128, 128), BF16), V((NY, 128, 512), F32),
            pltpu.SemaphoreType.DMA((SENDS,)),
            pltpu.SemaphoreType.DMA((COPIES,)),
            pltpu.SemaphoreType.DMA((LOCALS,)),
        ],
        compiler_params=pltpu.CompilerParams(
            collective_id=0, has_side_effects=True, vmem_limit_bytes=67000000
        ),
    )(
        tokens, retain_query, retain_key, retain_value, retain_gate, differ_query, differ_key,
        differ_value, retain_out, differ_out, log_decay[0].T, lambdas.reshape(1, 4), query_gain,
        key_gain, retain_gain.reshape(4, 128), differ_gain.reshape(4, 128), norm_gain.reshape(1, D),
        jnp.asarray(rope_tables()),
    )
    return (parts[0:1].astype(F32) + parts[1:2].astype(F32)).astype(BF16)


def solution(mesh):
    in_specs = (
        P("fs", "sp", "tp"), P(),
        P("fs", "tp"), P("fs", "tp"), P("fs", "tp"), P("fs", "tp"), P("fs", "tp"), P("fs", "tp"), P("fs", "tp"),
        P("fs", "sp", "tp"),
        P("tp"), P("tp", None, None), P("tp", None, None), P("tp"), P("tp"),
        P("tp", "fs"), P("tp", "fs"),
    )
    out_specs = P("fs", ("sp", "tp"), None)
    return jax.shard_map(body, mesh=mesh, in_specs=in_specs, out_specs=out_specs, check_vma=False)
```
